256 devices in a mesh: grp: 2 (over y), sp: 32 (over z, core), tp: 4 (over x).
Axes of the slice: x: 4, y: 2, z: 16, core: 2. Of those that a mesh axis runs over, the one named last changes fastest.
The devices are a block of a 4x16x16 slice.
Arguments:
- latents: bfloat16 [32768, 2048], P(('grp', 'sp', 'tp')), parts along dimension 0, may hold values from -6 to 6
- conv_value: bfloat16 [32768, 1024], P(('grp', 'sp'), 'tp'), parts along dimension 0, may hold values from -6 to 6
- conv_gate: bfloat16 [32768, 1024], P(('grp', 'sp'), 'tp'), parts along dimension 0, may hold values from -6 to 6
- conv_taps: float32 [31, 1024], P(None, 'tp'), may hold values from -2.2 to 2.2
- conv_gain: float32 [1024], P('tp'), may hold values from 0.1 to 1.9
- point_weight: bfloat16 [1024, 2048], P('tp'), may hold values from -0.1875 to 0.1875
- channel_gain: float32 [2048], replicated, may hold values from 0.1 to 1.9
- expert_ids: int32 [32768, 2], P(('grp', 'sp', 'tp')), parts along dimension 0, may hold values from 0 to 127, all different within a row; in each aligned block of 128 rows (0 to 127, 128 to 255, ...) at most 4 rows name the same one
- expert_weights: float32 [32768, 2], P(('grp', 'sp', 'tp')), parts along dimension 0, may hold values from 0.2 to 1
- gate_weight: bfloat16 [128, 2048, 768], P(('sp', 'tp')), may hold values from -0.125 to 0.125
- up_weight: bfloat16 [128, 2048, 768], P(('sp', 'tp')), may hold values from -0.125 to 0.125
- down_weight: bfloat16 [128, 768, 2048], P(('sp', 'tp')), may hold values from -0.21875 to 0.21875
Outputs:
- result: bfloat16 [32768, 2048], P(('grp', 'sp', 'tp')), parts along dimension 0
The draws below stay inside these ranges and needn't reach their ends.
There are 2 independent parts, one for each index of `grp`. The reference program is written for one: setup_inputs(seed, part) draws one part's arguments, and reference() takes and returns one part's arrays. A program takes and returns all parts, laid end to end along the dimension named above; an argument that names none is the same for every part. Nothing has to cross between parts.
Inputs may be any that keep to these rules, and one draw needn't show every extreme that they name: `expert_ids`: each row names 2 different experts. Within the rows of one device (aligned blocks of 128 rows) no expert is named by more than 4 rows, and in some device's rows some expert is named by exactly 4.
All inputs are finite; a program needn't handle non-finite values.
Results may differ from the reference program's by a relative error of at most 0.012.
Values may be sent and summed in bfloat16 or wider, within the bound.
No kernel may reach another device: no remote copies, remote signals or barrier semaphores. Data moves between devices by JAX's collectives and lax.ppermute only.
A program may use at most 64 MiB of HBM per device.

```python
import math
import jax
import jax.numpy as jnp
import numpy as np
from jax import lax

D = 2048
CONV_WIDTH = 1024
KERNEL = 31
EXPERT_WIDTH = 768
TOP_K = 2
TOK_DEV = 128
EXPERTS = 128
TOKENS = 16384
CAP = 4


def draw_conv_taps(key, part):
    first_key, second_key = jax.random.split(jax.random.fold_in(key, 11))
    base = jax.random.truncated_normal(first_key, -3.0, 3.0, (KERNEL, CONV_WIDTH), jnp.float32)
    block_logs = jax.random.uniform(second_key, (16,), jnp.float32, -1.38, 1.38)
    channel_scale = jnp.repeat(jnp.exp(block_logs), CONV_WIDTH // 16)
    return base * KERNEL ** (-0.5) * channel_scale[None, :]


def block_scale(key, shape, cuts, least, top_value):
    level = 1.0
    for position, parts in cuts:
        steps = jax.random.uniform(jax.random.fold_in(jax.random.fold_in(key, 6), position), (parts,), jnp.float32, least / len(cuts), top_value / len(cuts))
        level = level * jnp.repeat(jnp.exp(steps), shape[position] // parts).reshape((-1,) + (1,) * (len(shape) - 1 - position))
    return level


def deal_out(own_key, own, number, rows, number_of, top, bound, skew):
    sequence = jax.random.permutation(own_key, number_of)
    heavy_load, ordinary = portions_of(number_of, rows * top, bound, skew, True), portions_of(number_of, rows * top, bound, skew, False)
    places = jnp.arange(number_of)

    def named(tallies, rotation):
        used = int((tallies > 0).sum())
        fixed = max(1, used // 4)
        passed = fixed + (places - fixed + rotation * (used - fixed)) % max(1, number_of - fixed)
        return jnp.zeros((number_of,), jnp.int32).at[sequence[jnp.where(places < fixed, places, passed)]].set(jnp.asarray(tallies, jnp.int32))

    tallies = jnp.where(number % 4 == 0, named(heavy_load, number // 4), named(ordinary, number - number // 4 - 1))
    mixed = jax.random.permutation(jax.random.fold_in(own, 3), number_of)
    source_of, receiver = mixed[0:number_of // 2 * 2:2], mixed[1:number_of // 2 * 2:2]
    margin = jnp.minimum(tallies[source_of] - 1, bound - tallies[receiver]) // 2
    margin = jnp.where((source_of == sequence[0]) | (receiver == sequence[0]) | (tallies[receiver] == 0), 0, jnp.maximum(margin, 0))
    passed = jax.random.randint(jax.random.fold_in(own, 4), (number_of // 2,), 0, 1 << 20) % (margin + 1)
    tallies = tallies.at[source_of].add(-passed).at[receiver].add(passed)
    labels = jnp.searchsorted(jnp.cumsum(tallies), jnp.arange(rows * top), side="right").astype(jnp.int32)
    grid = labels.reshape(top, rows).T
    grid = grid[jax.random.permutation(jax.random.fold_in(own, 1), rows)]
    rotation = jax.random.randint(jax.random.fold_in(own, 2), (rows, 1), 0, top)
    return jnp.take_along_axis(grid, (jnp.arange(top)[None, :] + rotation) % top, axis=1)


def portions_of(amount, total, bound, slope, full):
    weights = [(1 << 20) // math.isqrt(grade ** slope) + 1 for grade in range(1, amount + 1)]
    largest = bound if full else min(bound, max(-(-total // amount), total * weights[0] // sum(weights)))
    least = 1 if total - largest >= amount - 1 else 0
    holding, rest = [largest] + [least] * (amount - 1), total - largest - least * (amount - 1)
    while rest > 0:
        free = [i for i in range(1, amount) if holding[i] < largest] or [i for i in range(1, amount) if holding[i] < bound]
        pool, remaining = sum([weights[i] for i in free]), rest
        for i in free:
            more = min(bound - holding[i], max(1, remaining * weights[i] // pool), rest)
            holding[i] = holding[i] + more
            rest = rest - more
    return np.array(holding)


def bell_draw(rng, extent, width, limit, pieces=(), kind=jnp.bfloat16):
    result = jax.random.normal(rng, extent, jnp.float32) * width
    if len(pieces) > 0:
        result = block_scale(rng, extent, pieces, -0.22, 0.18) * result
    return jnp.clip(result, min=-limit, max=limit).astype(kind)


def setup_inputs(seed: int = 0, part: int = 0) -> dict:
    splits = jax.random.split(jax.random.key(seed), 13)
    part_splits = jax.random.split(jax.random.fold_in(splits[12], part), 13)
    latents = bell_draw(part_splits[0], (TOKENS, D), 1.0, 6.0, ((0, 128),))
    conv_value = bell_draw(part_splits[1], (TOKENS, CONV_WIDTH), 1.0, 6.0, ((0, 32), (1, 4)))
    conv_gate = bell_draw(part_splits[2], (TOKENS, CONV_WIDTH), 1.0, 6.0, ((0, 32), (1, 4)))
    conv_taps = draw_conv_taps(jax.random.fold_in(splits[12], 71), part)
    conv_gain = jnp.clip(1.0 + 0.18 * jax.random.normal(splits[4], (CONV_WIDTH,), jnp.float32), 0.1, 1.9)
    point_weight = bell_draw(splits[5], (CONV_WIDTH, D), CONV_WIDTH ** -0.5, 0.1875, ((0, 4),))
    channel_gain = jnp.clip(1.0 + 0.18 * jax.random.normal(splits[6], (D,), jnp.float32), 0.1, 1.9)
    expert_ids_keys = jax.random.split(jax.random.fold_in(part_splits[7], 1), TOKENS // TOK_DEV)
    expert_ids_turns = jax.random.permutation(jax.random.fold_in(part_splits[7], 3), TOKENS // TOK_DEV)
    expert_ids = jax.vmap(lambda own, number: deal_out(jax.random.fold_in(part_splits[7], 2), own, number, TOK_DEV, EXPERTS, TOP_K, CAP, 2))(expert_ids_keys, expert_ids_turns).reshape((TOKENS, TOP_K))
    expert_weights = jnp.clip(0.2 + 0.8 * jax.random.uniform(part_splits[8], (TOKENS, TOP_K), jnp.float32) ** block_scale(part_splits[8], (TOKENS, TOP_K), ((0, 128),), -0.2, 0.2), 0.2, 1.0)
    gate_weight = bell_draw(splits[9], (EXPERTS, D, EXPERT_WIDTH), D ** -0.5, 0.125, ((0, 128),))
    up_weight = bell_draw(splits[10], (EXPERTS, D, EXPERT_WIDTH), D ** -0.5, 0.125, ((0, 128),))
    down_weight = bell_draw(splits[11], (EXPERTS, EXPERT_WIDTH, D), EXPERT_WIDTH ** -0.5, 0.21875, ((0, 128),))
    return dict(latents=latents, conv_value=conv_value, conv_gate=conv_gate, conv_taps=conv_taps, conv_gain=conv_gain, point_weight=point_weight, channel_gain=channel_gain, expert_ids=expert_ids, expert_weights=expert_weights, gate_weight=gate_weight, up_weight=up_weight, down_weight=down_weight)


def reference(latents, conv_value, conv_gate, conv_taps, conv_gain, point_weight, channel_gain, expert_ids, expert_weights, gate_weight, up_weight, down_weight):
    gated_value = (conv_value.astype(jnp.float32) * jax.nn.sigmoid(conv_gate.astype(jnp.float32))).astype(jnp.bfloat16)
    half_span = KERNEL // 2
    padded = jnp.pad(gated_value.astype(jnp.float32), ((half_span, half_span), (0, 0)))
    tap_values = conv_taps.astype(jnp.float32)
    mixed_rows = jnp.zeros(gated_value.shape, jnp.float32)
    for offset in range(KERNEL):
        mixed_rows = mixed_rows + tap_values[offset][None, :] * padded[offset:offset + TOKENS]
    center = lax.optimization_barrier(jnp.mean(mixed_rows, axis=1, keepdims=True))
    spread = lax.optimization_barrier(jnp.mean(mixed_rows * mixed_rows, axis=1, keepdims=True)) - center * center
    activated = jax.nn.silu((mixed_rows - center) * lax.rsqrt(spread + 0.05) * conv_gain.astype(jnp.float32)).astype(jnp.bfloat16)
    branch = jnp.dot(activated, point_weight, preferred_element_type=jnp.float32)
    after_conv = (latents.astype(jnp.float32) + branch).astype(jnp.bfloat16)
    after_wide = after_conv.astype(jnp.float32)
    scale_rows = lax.rsqrt(lax.optimization_barrier(jnp.mean(after_wide * after_wide, axis=1, keepdims=True)) + 0.01)
    expert_in = (after_wide * scale_rows * channel_gain.astype(jnp.float32)).astype(jnp.bfloat16)
    blocks = TOKENS // TOK_DEV
    expert_slots = blocks * CAP
    flat_ids = expert_ids.astype(jnp.int32).reshape(blocks, TOK_DEV * TOP_K)
    onehot = (flat_ids[:, :, None] == jnp.arange(EXPERTS, dtype=jnp.int32)[None, None, :]).astype(jnp.int32)
    earlier = lax.optimization_barrier(jnp.sum((jnp.cumsum(onehot, axis=1) - onehot) * onehot, axis=2))
    block_index = jnp.arange(blocks, dtype=jnp.int32)[:, None]
    target = (flat_ids * expert_slots + block_index * CAP + earlier).reshape(-1).astype(jnp.int32)
    token_index = jnp.repeat(jnp.arange(TOKENS, dtype=jnp.int32), TOP_K)
    slot_table = jnp.full((EXPERTS * expert_slots,), TOKENS, jnp.int32).at[target].set(token_index)
    slot_table = slot_table.reshape(EXPERTS, expert_slots)
    padded_in = jnp.concatenate([expert_in, jnp.zeros((1, expert_in.shape[1]), jnp.bfloat16)], axis=0)

    def one_expert(operands):
        row_index, gate_rows, up_rows, down_rows = operands
        chosen = padded_in[row_index]
        gate_part = jnp.dot(chosen, gate_rows, preferred_element_type=jnp.float32)
        up_part = jnp.dot(chosen, up_rows, preferred_element_type=jnp.float32)
        hidden = (jax.nn.silu(gate_part) * up_part).astype(jnp.bfloat16)
        return jnp.dot(hidden, down_rows, preferred_element_type=jnp.float32).astype(jnp.bfloat16)
    outputs = lax.map(one_expert, (slot_table, gate_weight, up_weight, down_weight))
    picked = outputs.reshape(EXPERTS * expert_slots, -1)[target].astype(jnp.float32).reshape(TOKENS, TOP_K, -1)
    routed = lax.optimization_barrier(jnp.sum(expert_weights.astype(jnp.float32)[:, :, None] * picked, axis=1))
    return (after_wide + routed).astype(jnp.bfloat16)
```

```python
import functools

import jax
import jax.numpy as jnp
from jax import lax
from jax.experimental import pallas as pl
from jax.experimental.pallas import tpu as pltpu
from jax.sharding import PartitionSpec as P


F32 = jnp.float32
BF16 = jnp.bfloat16
HALO = 16
LANES = 128
PACK = 8


def dot(a, b):
    return jnp.dot(a, b, preferred_element_type=F32)


def iota(shape, dim):
    return lax.broadcasted_iota(jnp.int32, shape, dim)


def gate(value, gating):
    return (value.astype(F32) * jax.nn.sigmoid(gating.astype(F32))).astype(BF16)


def conv_kernel(value_ref, gate_ref, low_ref, high_ref, taps_ref, gain_ref, out_ref, pad_ref):
    taps, width = taps_ref.shape
    rows = value_ref.shape[0]
    owners, owner_rows = out_ref.shape[0], out_ref.shape[1] - PACK
    step = 64
    for part in range(width // LANES):
        lanes = slice(part * LANES, (part + 1) * LANES)
        pad_ref[part, 0:HALO] = low_ref[:, lanes].astype(F32)
        pad_ref[part, HALO : HALO + rows] = gate(value_ref[:, lanes], gate_ref[:, lanes]).astype(F32)
        pad_ref[part, HALO + rows :] = high_ref[:, lanes].astype(F32)
        for start in range(0, rows, step):
            total = jnp.zeros((step, LANES), F32)
            for tap in range(taps):
                first = start + HALO - taps // 2 + tap
                total = total + taps_ref[tap : tap + 1, lanes] * pad_ref[part, first : first + step]
            owner, row = divmod(start, owner_rows)
            out_ref[owner, row : row + step, lanes] = total
    for owner in range(owners):
        out_ref[owner, owner_rows:, :] = jnp.broadcast_to(gain_ref[...], (PACK, width))


def slots(ids_ref, experts):
    tokens = ids_ref.shape[1]
    expert = iota((experts, tokens), 0)
    chosen = jnp.zeros((experts, tokens), F32)
    for k in range(ids_ref.shape[0]):
        chosen = jnp.where(ids_ref[k : k + 1, :] == expert, 1.0, chosen)
    before = (iota((tokens, tokens), 0) < iota((tokens, tokens), 1)).astype(F32).astype(BF16)
    earlier = dot(chosen.astype(BF16), before)
    return jnp.where(chosen > 0, earlier + 1.0, 0.0)


def dispatch_kernel(
    place_ref, mixed_ref, latents_ref, own_ref, a1_ref, a2_ref, a3_ref, b1_ref, b2_ref, b3_ref,
    gain_ref, ids_ref, after_ref, box_ref, act_ref, x_ref,
):
    owners, _, width = mixed_ref.shape
    rows, features = latents_ref.shape
    half_width = width // 2
    total = jnp.zeros((rows, 1), F32)
    squares = jnp.zeros((rows, 1), F32)
    for j in range(owners):
        block = mixed_ref[j, :rows, :]
        total = total + jnp.sum(block, axis=1, keepdims=True)
        squares = squares + jnp.sum(block * block, axis=1, keepdims=True)
    center = total / (owners * width)
    scale = lax.rsqrt(squares / (owners * width) - center * center + 0.05)
    for j in range(owners):
        value = (mixed_ref[j, :rows, :] - center) * scale * mixed_ref[j, rows : rows + 1, :]
        value = (value * jax.nn.sigmoid(value)).astype(BF16)
        act_ref[2 * j] = value[:, :half_width]
        act_ref[2 * j + 1] = value[:, half_width:]
    place, core = place_ref[0], place_ref[1]
    step = 512
    squares = jnp.zeros((rows, 1), F32)
    for start in range(0, features, step):
        cols = slice(start, start + step)
        branch = dot(act_ref[2 * place], own_ref[:half_width, cols])
        branch = branch + dot(act_ref[2 * place + 1], own_ref[half_width:, cols])
        for hop, near_ref, far_ref in ((1, a1_ref, b1_ref), (2, a2_ref, b2_ref), (3, a3_ref, b3_ref)):
            source = 2 * lax.rem(place - hop + owners, owners)
            branch = branch + dot(act_ref[source + core], near_ref[:, cols])
            branch = branch + dot(act_ref[source + 1 - core], far_ref[:, cols])
        after = (latents_ref[:, cols].astype(F32) + branch).astype(BF16)
        after_ref[:, cols] = after
        after = after.astype(F32)
        squares = squares + jnp.sum(after * after, axis=1, keepdims=True)
    scale = lax.rsqrt(squares / features + 0.01)
    parts, cap = x_ref.shape[0] // rows, PACK * rows // x_ref.shape[0]
    span = features // parts
    for part in range(parts):
        cols = slice(part * span, (part + 1) * span)
        value = after_ref[:, cols].astype(F32) * scale * gain_ref[:, cols]
        x_ref[part * rows : (part + 1) * rows] = value.astype(BF16)
    experts = box_ref.shape[0] // PACK
    slot = slots(ids_ref, experts).astype(BF16)
    block = 2 * LANES
    for start in range(0, box_ref.shape[0], block):
        row = iota((block, experts), 0) + start
        spread = ((row >> 3) == iota((block, experts), 1)).astype(F32).astype(BF16)
        wanted = dot(spread, slot)
        row = iota((block, rows), 0)
        hit = wanted == ((row & (cap - 1)) + 1).astype(F32)
        picks = [
            (hit & (((row & (PACK - 1)) // cap) == part)).astype(F32).astype(BF16)
            for part in range(parts)
        ]
        pick = jnp.concatenate(picks, axis=1)
        box_ref[start : start + block] = dot(pick, x_ref[...]).astype(BF16)


def shuffle_matrix(size, parts, inverse):
    cap = PACK // parts
    sources = size // PACK
    packed = iota((size, size), 0 if inverse else 1)
    split = iota((size, size), 1 if inverse else 0)
    source, part, slot = packed >> 3, (packed & (PACK - 1)) // cap, packed & (cap - 1)
    return ((part * sources + source) * cap + slot == split).astype(F32).astype(BF16)


def expert_kernel(
    in_ref, gate_hbm, up_hbm, down_hbm, out_ref, x_ref, gate_ref, up_ref, down_ref, hidden_ref, y_ref, sems
):
    copies = [
        pltpu.make_async_copy(gate_hbm, gate_ref, sems.at[0]),
        pltpu.make_async_copy(up_hbm, up_ref, sems.at[1]),
        pltpu.make_async_copy(down_hbm, down_ref, sems.at[2]),
    ]
    for copy in copies:
        copy.start()
    parts, rows, span = x_ref.shape
    block = 2 * LANES
    sub = block // parts
    forward = shuffle_matrix(block, parts, False)
    for i in range(in_ref.shape[0] // block):
        moved = dot(forward, in_ref[i * block : (i + 1) * block]).astype(BF16)
        for part in range(parts):
            x_ref[part, i * sub : (i + 1) * sub] = moved[part * sub : (part + 1) * sub]
    copies[0].wait()
    copies[1].wait()
    hidden_width = gate_ref.shape[1]
    tile = 256

    def inner(n, carry):
        cols = pl.ds(pl.multiple_of(n * tile, tile), tile)
        gated = jnp.zeros((rows, tile), F32)
        upped = jnp.zeros((rows, tile), F32)
        for part in range(parts):
            at = slice(part * span, (part + 1) * span)
            gated = gated + dot(x_ref[part], gate_ref[at, cols])
            upped = upped + dot(x_ref[part], up_ref[at, cols])
        hidden_ref[:, cols] = (gated * jax.nn.sigmoid(gated) * upped).astype(BF16)
        return carry

    lax.fori_loop(0, hidden_width // tile, inner, 0)
    copies[2].wait()
    for part in range(parts):

        def outer(n, carry, part=part):
            cols = pl.ds(pl.multiple_of(n * tile, tile), tile)
            weights = down_ref[:, pl.ds(pl.multiple_of(part * span + n * tile, tile), tile)]
            y_ref[part, :, cols] = dot(hidden_ref[...], weights).astype(BF16)
            return carry

        lax.fori_loop(0, span // tile, outer, 0)
    backward = shuffle_matrix(block, parts, True)
    for i in range(in_ref.shape[0] // block):
        stacked = jnp.concatenate(
            [y_ref[part, i * sub : (i + 1) * sub] for part in range(parts)], axis=0
        )
        out_ref[i * block : (i + 1) * block] = dot(backward, stacked).astype(BF16)


def combine_kernel(in_ref, after_ref, ids_ref, weights_ref, out_ref):
    rows, features = after_ref.shape
    size, span = in_ref.shape
    parts = features // span
    cap = PACK // parts
    experts = size // PACK
    slot = jnp.transpose(slots(ids_ref, experts)).astype(BF16)
    expert = iota((experts, rows), 0)
    weight = jnp.zeros((experts, rows), F32)
    for k in range(ids_ref.shape[0]):
        weight = jnp.where(ids_ref[k : k + 1, :] == expert, weights_ref[k : k + 1, :], weight)
    weight = jnp.transpose(weight)
    coarse = weight.astype(BF16)
    fine = (weight - coarse.astype(F32)).astype(BF16)
    spread = (iota((experts, size), 0) == (iota((experts, size), 1) >> 3)).astype(F32).astype(BF16)
    column = iota((rows, size), 1)
    hit = dot(slot, spread) == ((column & (cap - 1)) + 1).astype(F32)
    coarse = jnp.where(hit, dot(coarse, spread), 0.0)
    fine = jnp.where(hit, dot(fine, spread), 0.0)
    for part in range(parts):
        here = ((column & (PACK - 1)) // cap) == part
        factors = jnp.concatenate(
            [jnp.where(here, coarse, 0.0).astype(BF16), jnp.where(here, fine, 0.0).astype(BF16)], axis=0
        )
        sums = dot(factors, in_ref[...])
        cols = slice(part * span, (part + 1) * span)
        out_ref[:, cols] = (after_ref[:, cols].astype(F32) + (sums[:rows] + sums[rows:])).astype(BF16)


VMEM = pl.BlockSpec(memory_space=pltpu.VMEM)
SMEM = pl.BlockSpec(memory_space=pltpu.SMEM)
ANY = pl.BlockSpec(memory_space=pl.ANY)


def call(kernel, specs, outs, scratch, flops, size):
    return pl.pallas_call(
        kernel,
        in_specs=specs,
        out_specs=VMEM if not isinstance(outs, (list, tuple)) else [VMEM] * len(outs),
        out_shape=outs,
        scratch_shapes=scratch,
        compiler_params=pltpu.CompilerParams(vmem_limit_bytes=size << 20),
        cost_estimate=pl.CostEstimate(flops=flops, bytes_accessed=1 << 20, transcendentals=0),
    )


def shards(
    latents, conv_value, conv_gate, conv_taps, conv_gain, point_weight, channel_gain,
    expert_ids, expert_weights, gate_weight, up_weight, down_weight,
):
    shape = jax.ShapeDtypeStruct
    rows, features = latents.shape
    block_rows, width = conv_value.shape
    owners = lax.axis_size("tp")
    stages = lax.axis_size("sp")
    members = owners * stages
    top_count = expert_ids.shape[1]
    experts = gate_weight.shape[0] * members
    cap = 2 * top_count * rows // experts
    parts = PACK // cap
    span = features // parts

    ahead = [(i, i + 1) for i in range(stages - 1)]
    behind = [(i + 1, i) for i in range(stages - 1)]
    low = lax.ppermute(gate(conv_value[-HALO:], conv_gate[-HALO:]), "sp", ahead)
    high = lax.ppermute(gate(conv_value[:HALO], conv_gate[:HALO]), "sp", behind)

    place = lax.axis_index("tp")
    core = lax.rem(lax.axis_index("sp"), 2)
    half_width = width // 2
    half = lax.dynamic_slice_in_dim(point_weight, core * half_width, half_width, 0)
    swap = [(i, i ^ 1) for i in range(stages)]
    near = [
        lax.ppermute(half, "tp", [(i, (i + hop) % owners) for i in range(owners)])
        for hop in range(1, owners)
    ]
    far = [lax.ppermute(piece, "sp", swap) for piece in near]

    mixed = call(
        conv_kernel, [VMEM] * 6, shape((owners, rows + PACK, width), F32),
        [pltpu.VMEM((width // LANES, block_rows + 2 * HALO, LANES), F32)], 10**9, 16,
    )(conv_value, conv_gate, low, high, conv_taps, conv_gain[None, :])
    mixed = lax.all_to_all(mixed, "tp", split_axis=0, concat_axis=0, tiled=True)

    ids = expert_ids.T
    after, box = call(
        dispatch_kernel, [SMEM] + [VMEM] * 11,
        [shape((rows, features), BF16), shape((experts * PACK, span), BF16)],
        [pltpu.VMEM((2 * owners, rows, half_width), BF16), pltpu.VMEM((parts * rows, span), BF16)],
        10**9, 32,
    )(jnp.stack([place, core]), mixed, latents, point_weight, *near, *far, channel_gain[None, :], ids)

    box = box.reshape(members, PACK, span)
    arrived = lax.all_to_all(box, ("sp", "tp"), split_axis=0, concat_axis=0, tiled=True)
    hidden_width = gate_weight.shape[2]
    answer = call(
        expert_kernel, [VMEM] + [ANY] * 3, shape((members * PACK, span), BF16),
        [
            pltpu.VMEM((parts, members * cap, span), BF16),
            pltpu.VMEM((features, hidden_width), BF16),
            pltpu.VMEM((features, hidden_width), BF16),
            pltpu.VMEM((hidden_width, features), BF16),
            pltpu.VMEM((members * cap, hidden_width), BF16),
            pltpu.VMEM((parts, members * cap, span), BF16),
            pltpu.SemaphoreType.DMA((3,)),
        ],
        5 * 10**9, 40,
    )(arrived.reshape(members * PACK, span), gate_weight[0], up_weight[0], down_weight[0])
    answer = answer.reshape(members, PACK, span)
    returned = lax.all_to_all(answer, ("sp", "tp"), split_axis=0, concat_axis=0, tiled=True)
    return call(combine_kernel, [VMEM] * 4, shape((rows, features), BF16), [], 10**9, 32)(
        returned.reshape(experts * PACK, span), after, ids, expert_weights.T
    )


def solution(mesh):
    tokens = ("grp", "sp", "tp")
    return jax.shard_map(
        shards,
        mesh=mesh,
        in_specs=(
            P(tokens, None),
            P(("grp", "sp"), "tp"),
            P(("grp", "sp"), "tp"),
            P(None, "tp"),
            P("tp"),
            P("tp", None),
            P(),
            P(tokens, None),
            P(tokens, None),
            P(("sp", "tp"), None, None),
            P(("sp", "tp"), None, None),
            P(("sp", "tp"), None, None),
        ),
        out_specs=P(tokens, None),
        check_vma=False,
    )
```

```python
import jax
import jax.numpy as jnp
from jax import lax
from jax.experimental import pallas as pl
from jax.experimental.pallas import tpu as pltpu
from jax.sharding import PartitionSpec as P


F32 = jnp.float32
BF16 = jnp.bfloat16
HALO = 16
LANES = 128
PACK = 8


def dot(a, b):
    return jnp.dot(a, b, preferred_element_type=F32)


def iota(shape, dim):
    return lax.broadcasted_iota(jnp.int32, shape, dim)


def gate(value, gating):
    return (value.astype(F32) * jax.nn.sigmoid(gating.astype(F32))).astype(BF16)


def conv_kernel(rows_ref, low_ref, high_ref, table_ref, out_ref, pad_ref):
    taps, width = table_ref.shape[0] - 1, table_ref.shape[1]
    rows = rows_ref.shape[0]
    owners, owner_rows = out_ref.shape[0], out_ref.shape[1] - PACK
    step = 64
    parts = [slice(first, first + LANES) for first in range(0, width, LANES)]
    for part, lanes in enumerate(parts):
        pad_ref[part, 0:HALO] = low_ref[:, lanes].astype(F32)
        pad_ref[part, HALO : HALO + rows] = rows_ref[:, lanes].astype(F32)
        pad_ref[part, HALO + rows :] = high_ref[:, lanes].astype(F32)
    for part, lanes in enumerate(parts):
        for start in range(0, rows, step):
            total = jnp.zeros((step, LANES), F32)
            for tap in range(taps):
                first = start + HALO - taps // 2 + tap
                total = total + table_ref[tap : tap + 1, lanes] * pad_ref[part, first : first + step]
            owner, row = divmod(start, owner_rows)
            out_ref[owner, row : row + step, lanes] = total
    for owner in range(owners):
        out_ref[owner, owner_rows:, :] = jnp.broadcast_to(table_ref[taps:, :], (PACK, width))


def slots(ids_ref, experts):
    tokens = ids_ref.shape[1]
    expert = iota((experts, tokens), 0)
    chosen = jnp.zeros((experts, tokens), F32)
    for k in range(ids_ref.shape[0]):
        chosen = jnp.where(ids_ref[k : k + 1, :] == expert, 1.0, chosen)
    before = (iota((tokens, tokens), 0) < iota((tokens, tokens), 1)).astype(F32).astype(BF16)
    earlier = dot(chosen.astype(BF16), before)
    return jnp.where(chosen > 0, earlier + 1.0, 0.0)


def dispatch_kernel(
    place_ref, mixed_ref, latents_ref, own_ref, near_ref, swapped_ref, half_ref, rest_ref, gain_ref, ids_ref, after_ref, box_ref, act_ref, x_ref,
):
    owners, _, width = mixed_ref.shape
    rows, features = latents_ref.shape
    half_width = width // 2
    total = jnp.zeros((rows, 1), F32)
    squares = jnp.zeros((rows, 1), F32)
    for j in range(owners):
        block = mixed_ref[j, :rows, :]
        total = total + jnp.sum(block, axis=1, keepdims=True)
        squares = squares + jnp.sum(block * block, axis=1, keepdims=True)
    center = total / (owners * width)
    scale = lax.rsqrt(squares / (owners * width) - center * center + 0.05)
    for j in range(owners):
        value = (mixed_ref[j, :rows, :] - center) * scale * mixed_ref[j, rows : rows + 1, :]
        act_ref[j] = (value * jax.nn.sigmoid(value)).astype(BF16)
    place, core = place_ref[0], place_ref[1]
    before = lax.rem(place + owners - 1 + 2 * core, owners)
    beyond = lax.rem(place + owners + 1 - 2 * core, owners)
    across = act_ref[lax.rem(place + 2, owners)]
    lower, upper = across[:, :half_width], across[:, half_width:]
    first = jnp.where(core == 0, lower, upper)
    second = jnp.where(core == 0, upper, lower)
    step = 512
    squares = jnp.zeros((rows, 1), F32)
    for start in range(0, features, step):
        cols = slice(start, start + step)
        branch = dot(act_ref[place], own_ref[:, cols])
        branch = branch + dot(act_ref[before], near_ref[:, cols])
        branch = branch + dot(act_ref[beyond], swapped_ref[:, cols])
        branch = branch + dot(first, half_ref[:, cols]) + dot(second, rest_ref[:, cols])
        after = (latents_ref[:, cols].astype(F32) + branch).astype(BF16)
        after_ref[:, cols] = after
        after = after.astype(F32)
        squares = squares + jnp.sum(after * after, axis=1, keepdims=True)
    scale = lax.rsqrt(squares / features + 0.01)
    parts, cap = x_ref.shape[0] // rows, PACK * rows // x_ref.shape[0]
    span = features // parts
    for part in range(parts):
        cols = slice(part * span, (part + 1) * span)
        value = after_ref[:, cols].astype(F32) * scale * gain_ref[:, cols]
        x_ref[part * rows : (part + 1) * rows] = value.astype(BF16)
    experts = box_ref.shape[0] // PACK
    slot = slots(ids_ref, experts).astype(BF16)
    block = 2 * LANES
    for start in range(0, box_ref.shape[0], block):
        row = iota((block, experts), 0) + start
        spread = ((row >> 3) == iota((block, experts), 1)).astype(F32).astype(BF16)
        wanted = dot(spread, slot)
        row = iota((block, rows), 0)
        hit = wanted == ((row & (cap - 1)) + 1).astype(F32)
        picks = [
            (hit & (((row & (PACK - 1)) // cap) == part)).astype(F32).astype(BF16)
            for part in range(parts)
        ]
        pick = jnp.concatenate(picks, axis=1)
        box_ref[start : start + block] = dot(pick, x_ref[...]).astype(BF16)


def shuffle_matrix(size, parts, inverse):
    cap = PACK // parts
    sources = size // PACK
    packed = iota((size, size), 0 if inverse else 1)
    split = iota((size, size), 1 if inverse else 0)
    source, part, slot = packed >> 3, (packed & (PACK - 1)) // cap, packed & (cap - 1)
    return ((part * sources + source) * cap + slot == split).astype(F32).astype(BF16)


def expert_kernel(in_ref, gate_ref, up_ref, down_ref, out_ref, x_ref, hidden_ref, y_ref):
    parts, rows, span = x_ref.shape
    block = 2 * LANES
    sub = block // parts
    forward = shuffle_matrix(block, parts, False)
    for i in range(in_ref.shape[0] // block):
        moved = dot(forward, in_ref[i * block : (i + 1) * block]).astype(BF16)
        for part in range(parts):
            x_ref[part, i * sub : (i + 1) * sub] = moved[part * sub : (part + 1) * sub]
    hidden_width = gate_ref.shape[1]
    tile = 256

    def inner(n, carry):
        cols = pl.ds(pl.multiple_of(n * tile, tile), tile)
        gated = jnp.zeros((rows, tile), F32)
        upped = jnp.zeros((rows, tile), F32)
        for part in range(parts):
            at = slice(part * span, (part + 1) * span)
            gated = gated + dot(x_ref[part], gate_ref[at, cols])
            upped = upped + dot(x_ref[part], up_ref[at, cols])
        hidden_ref[:, cols] = (gated * jax.nn.sigmoid(gated) * upped).astype(BF16)
        return carry

    lax.fori_loop(0, hidden_width // tile, inner, 0)
    for part in range(parts):

        def outer(n, carry, part=part):
            cols = pl.ds(pl.multiple_of(n * tile, tile), tile)
            weights = down_ref[:, pl.ds(pl.multiple_of(part * span + n * tile, tile), tile)]
            y_ref[part, :, cols] = dot(hidden_ref[...], weights).astype(BF16)
            return carry

        lax.fori_loop(0, span // tile, outer, 0)
    backward = shuffle_matrix(block, parts, True)
    for i in range(in_ref.shape[0] // block):
        stacked = jnp.concatenate(
            [y_ref[part, i * sub : (i + 1) * sub] for part in range(parts)], axis=0
        )
        out_ref[i * block : (i + 1) * block] = dot(backward, stacked).astype(BF16)


def combine_kernel(in_ref, after_ref, ids_ref, weights_ref, out_ref):
    rows, features = after_ref.shape
    size, span = in_ref.shape
    parts = features // span
    cap = PACK // parts
    experts = size // PACK
    slot = jnp.transpose(slots(ids_ref, experts)).astype(BF16)
    expert = iota((experts, rows), 0)
    weight = jnp.zeros((experts, rows), F32)
    for k in range(ids_ref.shape[0]):
        weight = jnp.where(ids_ref[k : k + 1, :] == expert, weights_ref[k : k + 1, :], weight)
    weight = jnp.transpose(weight)
    coarse = weight.astype(BF16)
    fine = (weight - coarse.astype(F32)).astype(BF16)
    spread = (iota((experts, size), 0) == (iota((experts, size), 1) >> 3)).astype(F32).astype(BF16)
    column = iota((rows, size), 1)
    hit = dot(slot, spread) == ((column & (cap - 1)) + 1).astype(F32)
    coarse = jnp.where(hit, dot(coarse, spread), 0.0)
    fine = jnp.where(hit, dot(fine, spread), 0.0)
    for part in range(parts):
        here = ((column & (PACK - 1)) // cap) == part
        factors = jnp.concatenate(
            [jnp.where(here, coarse, 0.0).astype(BF16), jnp.where(here, fine, 0.0).astype(BF16)], axis=0
        )
        sums = dot(factors, in_ref[...])
        cols = slice(part * span, (part + 1) * span)
        out_ref[:, cols] = (after_ref[:, cols].astype(F32) + (sums[:rows] + sums[rows:])).astype(BF16)


VMEM = pl.BlockSpec(memory_space=pltpu.VMEM)
SMEM = pl.BlockSpec(memory_space=pltpu.SMEM)


def call(kernel, specs, outs, scratch, flops, size):
    return pl.pallas_call(
        kernel,
        in_specs=specs,
        out_specs=VMEM if not isinstance(outs, (list, tuple)) else [VMEM] * len(outs),
        out_shape=outs,
        scratch_shapes=scratch,
        compiler_params=pltpu.CompilerParams(vmem_limit_bytes=size << 20),
        cost_estimate=pl.CostEstimate(flops=flops, bytes_accessed=1 << 20, transcendentals=0),
    )


def shards(
    latents, conv_value, conv_gate, conv_taps, conv_gain, point_weight, channel_gain,
    expert_ids, expert_weights, gate_weight, up_weight, down_weight,
):
    shape = jax.ShapeDtypeStruct
    rows, features = latents.shape
    block_rows, width = conv_value.shape
    owners = lax.axis_size("tp")
    stages = lax.axis_size("sp")
    members = owners * stages
    top_count = expert_ids.shape[1]
    experts = gate_weight.shape[0] * members
    cap = 2 * top_count * rows // experts
    parts = PACK // cap
    span = features // parts

    ahead = [(i, i + 1) for i in range(stages - 1)]
    behind = [(i + 1, i) for i in range(stages - 1)]
    low = lax.ppermute(gate(conv_value[-HALO:], conv_gate[-HALO:]), "sp", ahead)
    high = lax.ppermute(gate(conv_value[:HALO], conv_gate[:HALO]), "sp", behind)

    place = lax.axis_index("tp")
    core = lax.rem(lax.axis_index("sp"), 2)
    half_width = width // 2
    aside = [
        (stage * owners + i, stage * owners + (i + (1, owners - 1)[stage % 2]) % owners)
        for stage in range(stages)
        for i in range(owners)
    ]
    opposite = [(i, (i + 2) % owners) for i in range(owners)]
    swap = [(i, i ^ 1) for i in range(stages)]
    near = lax.ppermute(point_weight, ("sp", "tp"), aside)
    half = lax.dynamic_slice_in_dim(point_weight, core * half_width, half_width, 0)
    half = lax.ppermute(half, "tp", opposite)

    gated = gate(conv_value, conv_gate)
    table = jnp.concatenate([conv_taps, conv_gain[None, :]], axis=0)
    mixed = call(
        conv_kernel, [VMEM] * 4, shape((owners, rows + PACK, width), F32),
        [pltpu.VMEM((width // LANES, block_rows + 2 * HALO, LANES), F32)], 10**9, 16,
    )(gated, low, high, table)
    near, half, _ = lax.optimization_barrier((near, half, mixed))
    swapped = lax.ppermute(near, "sp", swap)
    rest = lax.ppermute(half, "sp", swap)
    mixed = lax.all_to_all(mixed, "tp", split_axis=0, concat_axis=0, tiled=True)

    ids = expert_ids.T
    after, box = call(
        dispatch_kernel, [SMEM] + [VMEM] * 9,
        [shape((rows, features), BF16), shape((experts * PACK, span), BF16)],
        [pltpu.VMEM((owners, rows, width), BF16), pltpu.VMEM((parts * rows, span), BF16)],
        10**9, 32,
    )(jnp.stack([place, core]), mixed, latents, point_weight, near, swapped, half, rest, channel_gain[None, :], ids)

    box = box.reshape(members, PACK, span)
    arrived = lax.all_to_all(box, ("sp", "tp"), split_axis=0, concat_axis=0, tiled=True)
    hidden_width = gate_weight.shape[2]
    answer = call(
        expert_kernel, [VMEM] * 4, shape((members * PACK, span), BF16),
        [
            pltpu.VMEM((parts, members * cap, span), BF16),
            pltpu.VMEM((members * cap, hidden_width), BF16),
            pltpu.VMEM((parts, members * cap, span), BF16),
        ],
        5 * 10**9, 24,
    )(arrived.reshape(members * PACK, span), gate_weight[0], up_weight[0], down_weight[0])
    answer = answer.reshape(members, PACK, span)
    returned = lax.all_to_all(answer, ("sp", "tp"), split_axis=0, concat_axis=0, tiled=True)
    return call(combine_kernel, [VMEM] * 4, shape((rows, features), BF16), [], 10**9, 32)(
        returned.reshape(experts * PACK, span), after, ids, expert_weights.T
    )


def solution(mesh):
    tokens = ("grp", "sp", "tp")
    return jax.shard_map(
        shards,
        mesh=mesh,
        in_specs=(
            P(tokens, None),
            P(("grp", "sp"), "tp"),
            P(("grp", "sp"), "tp"),
            P(None, "tp"),
            P("tp"),
            P("tp", None),
            P(),
            P(tokens, None),
            P(tokens, None),
            P(("sp", "tp"), None, None),
            P(("sp", "tp"), None, None),
            P(("sp", "tp"), None, None),
        ),
        out_specs=P(tokens, None),
        check_vma=False,
    )
```

```python
import jax
import jax.numpy as jnp
from jax import lax
from jax.experimental import pallas as pl
from jax.experimental.pallas import tpu as pltpu
from jax.sharding import PartitionSpec as P


F32 = jnp.float32
BF16 = jnp.bfloat16
HALO = 16
LANES = 128
PACK = 8


def dot(a, b):
    return jnp.dot(a, b, preferred_element_type=F32)


def iota(shape, dim):
    return lax.broadcasted_iota(jnp.int32, shape, dim)


def gate(value, gating):
    return (value.astype(F32) * jax.nn.sigmoid(gating.astype(F32))).astype(BF16)


def conv_kernel(rows_ref, low_ref, high_ref, table_ref, out_ref, pad_ref):
    taps, width = table_ref.shape[0] - 1, table_ref.shape[1]
    rows = rows_ref.shape[0]
    owners, owner_rows = out_ref.shape[0], out_ref.shape[1] - PACK
    step = 64
    parts = [slice(first, first + LANES) for first in range(0, width, LANES)]
    for part, lanes in enumerate(parts):
        pad_ref[part, 0:HALO] = low_ref[:, lanes].astype(F32)
        pad_ref[part, HALO : HALO + rows] = rows_ref[:, lanes].astype(F32)
        pad_ref[part, HALO + rows :] = high_ref[:, lanes].astype(F32)
    for part, lanes in enumerate(parts):
        for start in range(0, rows, step):
            total = jnp.zeros((step, LANES), F32)
            for tap in range(taps):
                first = start + HALO - taps // 2 + tap
                total = total + table_ref[tap : tap + 1, lanes] * pad_ref[part, first : first + step]
            owner, row = divmod(start, owner_rows)
            out_ref[owner, row : row + step, lanes] = total
    for owner in range(owners):
        out_ref[owner, owner_rows:, :] = jnp.broadcast_to(table_ref[taps:, :], (PACK, width))


def slots(ids_ref, experts):
    tokens = ids_ref.shape[1]
    expert = iota((experts, tokens), 0)
    chosen = jnp.zeros((experts, tokens), F32)
    for k in range(ids_ref.shape[0]):
        chosen = jnp.where(ids_ref[k : k + 1, :] == expert, 1.0, chosen)
    before = (iota((tokens, tokens), 0) < iota((tokens, tokens), 1)).astype(F32).astype(BF16)
    earlier = dot(chosen.astype(BF16), before)
    return jnp.where(chosen > 0, earlier + 1.0, 0.0)


def dispatch_kernel(
    place_ref, mixed_ref, latents_ref, own_ref, near_ref, swapped_ref, half_ref, rest_ref, gain_ref, ids_ref, after_ref, box_ref, act_ref, x_ref,
):
    owners, _, width = mixed_ref.shape
    rows, features = latents_ref.shape
    half_width = width // 2
    total = jnp.zeros((rows, 1), F32)
    squares = jnp.zeros((rows, 1), F32)
    for j in range(owners):
        block = mixed_ref[j, :rows, :]
        total = total + jnp.sum(block, axis=1, keepdims=True)
        squares = squares + jnp.sum(block * block, axis=1, keepdims=True)
    center = total / (owners * width)
    scale = lax.rsqrt(squares / (owners * width) - center * center + 0.05)
    for j in range(owners):
        value = (mixed_ref[j, :rows, :] - center) * scale * mixed_ref[j, rows : rows + 1, :]
        act_ref[j] = (value * jax.nn.sigmoid(value)).astype(BF16)
    place, core = place_ref[0], place_ref[1]
    before = lax.rem(place + owners - 1 + 2 * core, owners)
    beyond = lax.rem(place + owners + 1 - 2 * core, owners)
    across = act_ref[lax.rem(place + 2, owners)]
    lower, upper = across[:, :half_width], across[:, half_width:]
    first = jnp.where(core == 0, lower, upper)
    second = jnp.where(core == 0, upper, lower)
    step = 512
    squares = jnp.zeros((rows, 1), F32)
    for start in range(0, features, step):
        cols = slice(start, start + step)
        branch = dot(act_ref[place], own_ref[:, cols])
        branch = branch + dot(act_ref[before], near_ref[:, cols])
        branch = branch + dot(act_ref[beyond], swapped_ref[:, cols])
        branch = branch + dot(first, half_ref[:, cols]) + dot(second, rest_ref[:, cols])
        after = (latents_ref[:, cols].astype(F32) + branch).astype(BF16)
        after_ref[:, cols] = after
        after = after.astype(F32)
        squares = squares + jnp.sum(after * after, axis=1, keepdims=True)
    scale = lax.rsqrt(squares / features + 0.01)
    parts, cap = x_ref.shape[0] // rows, PACK * rows // x_ref.shape[0]
    span = features // parts
    for part in range(parts):
        cols = slice(part * span, (part + 1) * span)
        value = after_ref[:, cols].astype(F32) * scale * gain_ref[:, cols]
        x_ref[part * rows : (part + 1) * rows] = value.astype(BF16)
    experts = box_ref.shape[0] // PACK
    slot = slots(ids_ref, experts).astype(BF16)
    block = 2 * LANES
    for start in range(0, box_ref.shape[0], block):
        row = iota((block, experts), 0) + start
        spread = ((row >> 3) == iota((block, experts), 1)).astype(F32).astype(BF16)
        wanted = dot(spread, slot)
        row = iota((block, rows), 0)
        hit = wanted == ((row & (cap - 1)) + 1).astype(F32)
        picks = [
            (hit & (((row & (PACK - 1)) // cap) == part)).astype(F32).astype(BF16)
            for part in range(parts)
        ]
        pick = jnp.concatenate(picks, axis=1)
        box_ref[start : start + block] = dot(pick, x_ref[...]).astype(BF16)


def shuffle_matrix(size, parts, inverse):
    cap = PACK // parts
    sources = size // PACK
    packed = iota((size, size), 0 if inverse else 1)
    split = iota((size, size), 1 if inverse else 0)
    source, part, slot = packed >> 3, (packed & (PACK - 1)) // cap, packed & (cap - 1)
    return ((part * sources + source) * cap + slot == split).astype(F32).astype(BF16)


def expert_kernel(in_ref, gate_ref, up_ref, down_ref, out_ref, x_ref, hidden_ref, y_ref):
    parts, rows, span = x_ref.shape
    block = 2 * LANES
    sub = block // parts
    forward = shuffle_matrix(block, parts, False)
    for i in range(in_ref.shape[0] // block):
        moved = dot(forward, in_ref[i * block : (i + 1) * block]).astype(BF16)
        for part in range(parts):
            x_ref[part, i * sub : (i + 1) * sub] = moved[part * sub : (part + 1) * sub]
    hidden_width = gate_ref.shape[1]
    tile = 256

    def inner(n, carry):
        cols = pl.ds(pl.multiple_of(n * tile, tile), tile)
        gated = jnp.zeros((rows, tile), F32)
        upped = jnp.zeros((rows, tile), F32)
        for part in range(parts):
            at = slice(part * span, (part + 1) * span)
            gated = gated + dot(x_ref[part], gate_ref[at, cols])
            upped = upped + dot(x_ref[part], up_ref[at, cols])
        hidden_ref[:, cols] = (gated * jax.nn.sigmoid(gated) * upped).astype(BF16)
        return carry

    lax.fori_loop(0, hidden_width // tile, inner, 0, unroll=True)
    for part in range(parts):

        def outer(n, carry, part=part):
            cols = pl.ds(pl.multiple_of(n * tile, tile), tile)
            weights = down_ref[:, pl.ds(pl.multiple_of(part * span + n * tile, tile), tile)]
            y_ref[part, :, cols] = dot(hidden_ref[...], weights).astype(BF16)
            return carry

        lax.fori_loop(0, span // tile, outer, 0, unroll=True)
    backward = shuffle_matrix(block, parts, True)
    for i in range(in_ref.shape[0] // block):
        stacked = jnp.concatenate(
            [y_ref[part, i * sub : (i + 1) * sub] for part in range(parts)], axis=0
        )
        out_ref[i * block : (i + 1) * block] = dot(backward, stacked).astype(BF16)


def combine_kernel(in_ref, after_ref, ids_ref, weights_ref, out_ref):
    rows, features = after_ref.shape
    size, span = in_ref.shape
    parts = features // span
    cap = PACK // parts
    experts = size // PACK
    slot = jnp.transpose(slots(ids_ref, experts)).astype(BF16)
    expert = iota((experts, rows), 0)
    weight = jnp.zeros((experts, rows), F32)
    for k in range(ids_ref.shape[0]):
        weight = jnp.where(ids_ref[k : k + 1, :] == expert, weights_ref[k : k + 1, :], weight)
    weight = jnp.transpose(weight)
    coarse = weight.astype(BF16)
    fine = (weight - coarse.astype(F32)).astype(BF16)
    spread = (iota((experts, size), 0) == (iota((experts, size), 1) >> 3)).astype(F32).astype(BF16)
    column = iota((rows, size), 1)
    hit = dot(slot, spread) == ((column & (cap - 1)) + 1).astype(F32)
    coarse = jnp.where(hit, dot(coarse, spread), 0.0)
    fine = jnp.where(hit, dot(fine, spread), 0.0)
    for part in range(parts):
        here = ((column & (PACK - 1)) // cap) == part
        factors = jnp.concatenate(
            [jnp.where(here, coarse, 0.0).astype(BF16), jnp.where(here, fine, 0.0).astype(BF16)], axis=0
        )
        sums = dot(factors, in_ref[...])
        cols = slice(part * span, (part + 1) * span)
        out_ref[:, cols] = (after_ref[:, cols].astype(F32) + (sums[:rows] + sums[rows:])).astype(BF16)


VMEM = pl.BlockSpec(memory_space=pltpu.VMEM)
SMEM = pl.BlockSpec(memory_space=pltpu.SMEM)


def call(kernel, specs, outs, scratch, flops, size):
    return pl.pallas_call(
        kernel,
        in_specs=specs,
        out_specs=VMEM if not isinstance(outs, (list, tuple)) else [VMEM] * len(outs),
        out_shape=outs,
        scratch_shapes=scratch,
        compiler_params=pltpu.CompilerParams(vmem_limit_bytes=size << 20),
        cost_estimate=pl.CostEstimate(flops=flops, bytes_accessed=1 << 20, transcendentals=0),
    )


def shards(
    latents, conv_value, conv_gate, conv_taps, conv_gain, point_weight, channel_gain,
    expert_ids, expert_weights, gate_weight, up_weight, down_weight,
):
    shape = jax.ShapeDtypeStruct
    rows, features = latents.shape
    block_rows, width = conv_value.shape
    owners = lax.axis_size("tp")
    stages = lax.axis_size("sp")
    members = owners * stages
    top_count = expert_ids.shape[1]
    experts = gate_weight.shape[0] * members
    cap = 2 * top_count * rows // experts
    parts = PACK // cap
    span = features // parts

    ahead = [(i, i + 1) for i in range(stages - 1)]
    behind = [(i + 1, i) for i in range(stages - 1)]
    low = lax.ppermute(gate(conv_value[-HALO:], conv_gate[-HALO:]), "sp", ahead)
    high = lax.ppermute(gate(conv_value[:HALO], conv_gate[:HALO]), "sp", behind)

    place = lax.axis_index("tp")
    core = lax.rem(lax.axis_index("sp"), 2)
    half_width = width // 2
    aside = [
        (stage * owners + i, stage * owners + (i + (1, owners - 1)[stage % 2]) % owners)
        for stage in range(stages)
        for i in range(owners)
    ]
    swap = [(i, i ^ 1) for i in range(stages)]
    near = lax.ppermute(point_weight, ("sp", "tp"), aside)

    gated = gate(conv_value, conv_gate)
    table = jnp.concatenate([conv_taps, conv_gain[None, :]], axis=0)
    mixed = call(
        conv_kernel, [VMEM] * 4, shape((owners, rows + PACK, width), F32),
        [pltpu.VMEM((width // LANES, block_rows + 2 * HALO, LANES), F32)], 10**9, 16,
    )(gated, low, high, table)
    near, _ = lax.optimization_barrier((near, mixed))
    half = lax.dynamic_slice_in_dim(near, core * half_width, half_width, 0)
    half = lax.ppermute(half, ("sp", "tp"), aside)
    swapped = lax.ppermute(near, "sp", swap)
    rest = lax.ppermute(half, "sp", swap)
    mixed = lax.all_to_all(mixed, "tp", split_axis=0, concat_axis=0, tiled=True)

    ids = expert_ids.T
    after, box = call(
        dispatch_kernel, [SMEM] + [VMEM] * 9,
        [shape((rows, features), BF16), shape((experts * PACK, span), BF16)],
        [pltpu.VMEM((owners, rows, width), BF16), pltpu.VMEM((parts * rows, span), BF16)],
        10**9, 32,
    )(jnp.stack([place, core]), mixed, latents, point_weight, near, swapped, half, rest, channel_gain[None, :], ids)

    box = box.reshape(members, PACK, span)
    arrived = lax.all_to_all(box, ("sp", "tp"), split_axis=0, concat_axis=0, tiled=True)
    hidden_width = gate_weight.shape[2]
    answer = call(
        expert_kernel, [VMEM] * 4, shape((members * PACK, span), BF16),
        [
            pltpu.VMEM((parts, members * cap, span), BF16),
            pltpu.VMEM((members * cap, hidden_width), BF16),
            pltpu.VMEM((parts, members * cap, span), BF16),
        ],
        5 * 10**9, 24,
    )(arrived.reshape(members * PACK, span), gate_weight[0], up_weight[0], down_weight[0])
    answer = answer.reshape(members, PACK, span)
    returned = lax.all_to_all(answer, ("sp", "tp"), split_axis=0, concat_axis=0, tiled=True)
    return call(combine_kernel, [VMEM] * 4, shape((rows, features), BF16), [], 10**9, 32)(
        returned.reshape(experts * PACK, span), after, ids, expert_weights.T
    )


def solution(mesh):
    tokens = ("grp", "sp", "tp")
    return jax.shard_map(
        shards,
        mesh=mesh,
        in_specs=(
            P(tokens, None),
            P(("grp", "sp"), "tp"),
            P(("grp", "sp"), "tp"),
            P(None, "tp"),
            P("tp"),
            P("tp", None),
            P(),
            P(tokens, None),
            P(tokens, None),
            P(("sp", "tp"), None, None),
            P(("sp", "tp"), None, None),
            P(("sp", "tp"), None, None),
        ),
        out_specs=P(tokens, None),
        check_vma=False,
    )
```

```python
import jax
import jax.numpy as jnp
from jax import lax
from jax.experimental import pallas as pl
from jax.experimental.pallas import tpu as pltpu
from jax.sharding import PartitionSpec as P


F32 = jnp.float32
BF16 = jnp.bfloat16
HALO = 16
LANES = 128
PACK = 8
EXTRA = 16


def dot(a, b):
    return jnp.dot(a, b, preferred_element_type=F32)


def iota(shape, dim):
    return lax.broadcasted_iota(jnp.int32, shape, dim)


def gate(value, gating):
    return (value.astype(F32) * jax.nn.sigmoid(gating.astype(F32))).astype(BF16)


def terms(value):
    high = value.astype(BF16)
    rest = value - high.astype(F32)
    middle = rest.astype(BF16)
    return high, middle, (rest - middle.astype(F32)).astype(BF16)


def joined(block_ref, j, first):
    rows = [block_ref[j, first + k : first + k + 1, :].astype(F32) for k in range(3)]
    return rows[0] + rows[1] + rows[2]


def conv_kernel(rows_ref, low_ref, high_ref, table_ref, out_ref, pad_ref, sum_ref):
    taps, width = table_ref.shape[0] - 1, table_ref.shape[1]
    rows = rows_ref.shape[0]
    owners, owner_rows = out_ref.shape[0], out_ref.shape[1] - EXTRA
    step = 64
    parts = [slice(first, first + LANES) for first in range(0, width, LANES)]
    for part, lanes in enumerate(parts):
        pad_ref[part, 0:HALO] = low_ref[:, lanes].astype(F32)
        pad_ref[part, HALO : HALO + rows] = rows_ref[:, lanes].astype(F32)
        pad_ref[part, HALO + rows :] = high_ref[:, lanes].astype(F32)
    for part, lanes in enumerate(parts):
        for start in range(0, rows, step):
            total = jnp.zeros((step, LANES), F32)
            for tap in range(taps):
                first = start + HALO - taps // 2 + tap
                total = total + table_ref[tap : tap + 1, lanes] * pad_ref[part, first : first + step]
            sum_ref[start : start + step, lanes] = total
    gains = terms(table_ref[taps:, :])
    spare = jnp.zeros((EXTRA - 6, width), BF16)
    for owner in range(owners):
        block = sum_ref[owner * owner_rows : (owner + 1) * owner_rows]
        mean = jnp.sum(block, axis=1, keepdims=True) / width
        out_ref[owner, :owner_rows] = (block - mean).astype(BF16)
        across = jnp.transpose(jnp.broadcast_to(mean, (owner_rows, owner_rows)))[:1]
        across = jnp.concatenate([across, jnp.zeros((1, width - owner_rows), F32)], axis=1)
        out_ref[owner, owner_rows:] = jnp.concatenate([*gains, *terms(across), spare], axis=0)


def slots(ids_ref, experts):
    tokens = ids_ref.shape[1]
    expert = iota((experts, tokens), 0)
    chosen = jnp.zeros((experts, tokens), F32)
    for k in range(ids_ref.shape[0]):
        chosen = jnp.where(ids_ref[k : k + 1, :] == expert, 1.0, chosen)
    before = (iota((tokens, tokens), 0) < iota((tokens, tokens), 1)).astype(F32).astype(BF16)
    earlier = dot(chosen.astype(BF16), before)
    return jnp.where(chosen > 0, earlier + 1.0, 0.0)


def routing_kernel(ids_ref, weights_ref, pick_ref, factor_ref):
    rows = ids_ref.shape[1]
    size = pick_ref.shape[0]
    parts = pick_ref.shape[1] // rows
    cap = PACK // parts
    experts = size // PACK
    slot = slots(ids_ref, experts)
    expert = iota((experts, rows), 0)
    weight = jnp.zeros((experts, rows), F32)
    for k in range(ids_ref.shape[0]):
        weight = jnp.where(ids_ref[k : k + 1, :] == expert, weights_ref[k : k + 1, :], weight)
    weight = jnp.transpose(weight)
    coarse = weight.astype(BF16)
    fine = (weight - coarse.astype(F32)).astype(BF16)
    across = jnp.transpose(slot).astype(BF16)
    slot = slot.astype(BF16)
    block = 2 * LANES
    for start in range(0, size, block):
        row = iota((block, experts), 0) + start
        spread = ((row >> 3) == iota((block, experts), 1)).astype(F32).astype(BF16)
        wanted = dot(spread, slot)
        row = iota((block, rows), 0)
        hit = wanted == ((row & (cap - 1)) + 1).astype(F32)
        for part in range(parts):
            here = hit & (((row & (PACK - 1)) // cap) == part)
            pick_ref[start : start + block, part * rows : (part + 1) * rows] = here.astype(F32).astype(BF16)
    spread = (iota((experts, size), 0) == (iota((experts, size), 1) >> 3)).astype(F32).astype(BF16)
    column = iota((rows, size), 1)
    hit = dot(across, spread) == ((column & (cap - 1)) + 1).astype(F32)
    coarse, fine = dot(coarse, spread), dot(fine, spread)
    for part in range(parts):
        here = hit & (((column & (PACK - 1)) // cap) == part)
        for k, value in enumerate((coarse, fine)):
            first = (2 * part + k) * rows
            factor_ref[first : first + rows] = jnp.where(here, value, 0.0).astype(BF16)


def partial_kernel(place_ref, mixed_ref, own_ref, near_ref, swapped_ref, half_ref, out_ref, rest_ref, value_ref, act_ref):
    owners, _, width = mixed_ref.shape
    rows, features = out_ref.shape
    half_width = width // 2
    total = jnp.zeros((rows, 1), F32)
    for j in range(owners):
        across = joined(mixed_ref, j, rows + 3)[:, :rows]
        mean = jnp.transpose(jnp.broadcast_to(across, (rows, rows)))[:, :1]
        value_ref[j] = mixed_ref[j, :rows, :].astype(F32) + mean
        total = total + jnp.sum(value_ref[j], axis=1, keepdims=True)
    center = total / (owners * width)
    squares = jnp.zeros((rows, 1), F32)
    for j in range(owners):
        value = value_ref[j] - center
        squares = squares + jnp.sum(value * value, axis=1, keepdims=True)
    scale = lax.rsqrt(squares / (owners * width) + 0.05)
    for j in range(owners):
        value = (value_ref[j] - center) * scale * joined(mixed_ref, j, rows)
        act_ref[j] = (value * jax.nn.sigmoid(value)).astype(BF16)
    place, core = place_ref[0], place_ref[1]
    before = lax.rem(place + owners - 1 + 2 * core, owners)
    beyond = lax.rem(place + owners + 1 - 2 * core, owners)
    across = act_ref[lax.rem(place + 2, owners)]
    lower, upper = across[:, :half_width], across[:, half_width:]
    first = jnp.where(core == 0, lower, upper)
    rest_ref[...] = jnp.where(core == 0, upper, lower)
    step = 512
    for start in range(0, features, step):
        cols = slice(start, start + step)
        branch = dot(act_ref[place], own_ref[:, cols])
        branch = branch + dot(act_ref[before], near_ref[:, cols])
        branch = branch + dot(act_ref[beyond], swapped_ref[:, cols])
        out_ref[:, cols] = branch + dot(first, half_ref[:, cols])


def dispatch_kernel(
    latents_ref, partial_ref, act_ref, rest_ref, gain_ref, pick_ref, after_ref, box_ref, x_ref
):
    rows, features = latents_ref.shape
    step = 512
    squares = jnp.zeros((rows, 1), F32)
    for start in range(0, features, step):
        cols = slice(start, start + step)
        branch = partial_ref[:, cols] + dot(act_ref[...], rest_ref[:, cols])
        after = (latents_ref[:, cols].astype(F32) + branch).astype(BF16)
        after_ref[:, cols] = after
        after = after.astype(F32)
        squares = squares + jnp.sum(after * after, axis=1, keepdims=True)
    scale = lax.rsqrt(squares / features + 0.01)
    parts = x_ref.shape[0] // rows
    span = features // parts
    for part in range(parts):
        cols = slice(part * span, (part + 1) * span)
        value = after_ref[:, cols].astype(F32) * scale * gain_ref[:, cols]
        x_ref[part * rows : (part + 1) * rows] = value.astype(BF16)
    block = 2 * LANES
    for start in range(0, box_ref.shape[0], block):
        box_ref[start : start + block] = dot(pick_ref[start : start + block], x_ref[...]).astype(BF16)


def shuffle_matrix(size, parts, inverse):
    cap = PACK // parts
    sources = size // PACK
    packed = iota((size, size), 0 if inverse else 1)
    split = iota((size, size), 1 if inverse else 0)
    source, part, slot = packed >> 3, (packed & (PACK - 1)) // cap, packed & (cap - 1)
    return ((part * sources + source) * cap + slot == split).astype(F32).astype(BF16)


def expert_kernel(in_ref, gate_ref, up_ref, down_ref, out_ref, x_ref, hidden_ref, y_ref):
    parts, rows, span = x_ref.shape
    block = 2 * LANES
    sub = block // parts
    forward = shuffle_matrix(block, parts, False)
    for i in range(in_ref.shape[0] // block):
        moved = dot(forward, in_ref[i * block : (i + 1) * block]).astype(BF16)
        for part in range(parts):
            x_ref[part, i * sub : (i + 1) * sub] = moved[part * sub : (part + 1) * sub]
    hidden_width = gate_ref.shape[1]
    tile = 256

    def inner(n, carry):
        cols = pl.ds(pl.multiple_of(n * tile, tile), tile)
        gated = jnp.zeros((rows, tile), F32)
        upped = jnp.zeros((rows, tile), F32)
        for part in range(parts):
            at = slice(part * span, (part + 1) * span)
            gated = gated + dot(x_ref[part], gate_ref[at, cols])
            upped = upped + dot(x_ref[part], up_ref[at, cols])
        hidden_ref[:, cols] = (gated * jax.nn.sigmoid(gated) * upped).astype(BF16)
        return carry

    lax.fori_loop(0, hidden_width // tile, inner, 0, unroll=True)
    for part in range(parts):

        def outer(n, carry, part=part):
            cols = pl.ds(pl.multiple_of(n * tile, tile), tile)
            weights = down_ref[:, pl.ds(pl.multiple_of(part * span + n * tile, tile), tile)]
            y_ref[part, :, cols] = dot(hidden_ref[...], weights).astype(BF16)
            return carry

        lax.fori_loop(0, span // tile, outer, 0, unroll=True)
    backward = shuffle_matrix(block, parts, True)
    for i in range(in_ref.shape[0] // block):
        stacked = jnp.concatenate(
            [y_ref[part, i * sub : (i + 1) * sub] for part in range(parts)], axis=0
        )
        out_ref[i * block : (i + 1) * block] = dot(backward, stacked).astype(BF16)


def combine_kernel(in_ref, after_ref, factor_ref, out_ref):
    rows, features = after_ref.shape
    span = in_ref.shape[1]
    for part in range(features // span):
        sums = dot(factor_ref[2 * part * rows : 2 * (part + 1) * rows], in_ref[...])
        cols = slice(part * span, (part + 1) * span)
        out_ref[:, cols] = (after_ref[:, cols].astype(F32) + (sums[:rows] + sums[rows:])).astype(BF16)


VMEM = pl.BlockSpec(memory_space=pltpu.VMEM)
SMEM = pl.BlockSpec(memory_space=pltpu.SMEM)


def call(kernel, specs, outs, scratch, flops, size):
    return pl.pallas_call(
        kernel,
        in_specs=specs,
        out_specs=VMEM if not isinstance(outs, (list, tuple)) else [VMEM] * len(outs),
        out_shape=outs,
        scratch_shapes=scratch,
        compiler_params=pltpu.CompilerParams(vmem_limit_bytes=size << 20),
        cost_estimate=pl.CostEstimate(flops=flops, bytes_accessed=1 << 20, transcendentals=0),
    )


def shards(
    latents, conv_value, conv_gate, conv_taps, conv_gain, point_weight, channel_gain,
    expert_ids, expert_weights, gate_weight, up_weight, down_weight,
):
    shape = jax.ShapeDtypeStruct
    rows, features = latents.shape
    block_rows, width = conv_value.shape
    owners = lax.axis_size("tp")
    stages = lax.axis_size("sp")
    members = owners * stages
    top_count = expert_ids.shape[1]
    experts = gate_weight.shape[0] * members
    cap = 2 * top_count * rows // experts
    parts = PACK // cap
    span = features // parts

    ahead = [(i, i + 1) for i in range(stages - 1)]
    behind = [(i + 1, i) for i in range(stages - 1)]
    low = lax.ppermute(gate(conv_value[-HALO:], conv_gate[-HALO:]), "sp", ahead)
    high = lax.ppermute(gate(conv_value[:HALO], conv_gate[:HALO]), "sp", behind)

    place = lax.axis_index("tp")
    core = lax.rem(lax.axis_index("sp"), 2)
    half_width = width // 2
    aside = [
        (stage * owners + i, stage * owners + (i + (1, owners - 1)[stage % 2]) % owners)
        for stage in range(stages)
        for i in range(owners)
    ]
    swap = [(i, i ^ 1) for i in range(stages)]
    near = lax.ppermute(point_weight, ("sp", "tp"), aside)

    gated = gate(conv_value, conv_gate)
    table = jnp.concatenate([conv_taps, conv_gain[None, :]], axis=0)
    sent = call(
        conv_kernel, [VMEM] * 4, shape((owners, rows + EXTRA, width), BF16),
        [
            pltpu.VMEM((width // LANES, block_rows + 2 * HALO, LANES), F32),
            pltpu.VMEM((block_rows, width), F32),
        ],
        10**9, 8,
    )(gated, low, high, table)
    near, _ = lax.optimization_barrier((near, sent))
    half = lax.dynamic_slice_in_dim(near, core * half_width, half_width, 0)
    half = lax.ppermute(half, ("sp", "tp"), aside)
    swapped = lax.ppermute(near, "sp", swap)
    rest = lax.ppermute(half, "sp", swap)
    mixed = lax.all_to_all(sent, "tp", split_axis=0, concat_axis=0, tiled=True)

    ids, weights, _ = lax.optimization_barrier((expert_ids.T, expert_weights.T, sent))
    pick, factor = call(
        routing_kernel, [VMEM] * 2,
        [shape((experts * PACK, parts * rows), BF16), shape((2 * parts * rows, experts * PACK), BF16)],
        [], 10**9, 8,
    )(ids, weights)
    partial, act = call(
        partial_kernel, [SMEM] + [VMEM] * 5,
        [shape((rows, features), F32), shape((rows, half_width), BF16)],
        [pltpu.VMEM((owners, rows, width), F32), pltpu.VMEM((owners, rows, width), BF16)],
        10**9, 8,
    )(jnp.stack([place, core]), mixed, point_weight, near, swapped, half)
    after, box = call(
        dispatch_kernel, [VMEM] * 6,
        [shape((rows, features), BF16), shape((experts * PACK, span), BF16)],
        [pltpu.VMEM((parts * rows, span), BF16)], 10**9, 8,
    )(latents, partial, act, rest, channel_gain[None, :], pick)

    box = box.reshape(members, PACK, span)
    arrived = lax.all_to_all(box, ("sp", "tp"), split_axis=0, concat_axis=0, tiled=True)
    hidden_width = gate_weight.shape[2]
    answer = call(
        expert_kernel, [VMEM] * 4, shape((members * PACK, span), BF16),
        [
            pltpu.VMEM((parts, members * cap, span), BF16),
            pltpu.VMEM((members * cap, hidden_width), BF16),
            pltpu.VMEM((parts, members * cap, span), BF16),
        ],
        5 * 10**9, 12,
    )(arrived.reshape(members * PACK, span), gate_weight[0], up_weight[0], down_weight[0])
    answer = answer.reshape(members, PACK, span)
    returned = lax.all_to_all(answer, ("sp", "tp"), split_axis=0, concat_axis=0, tiled=True)
    return call(combine_kernel, [VMEM] * 3, shape((rows, features), BF16), [], 10**9, 8)(
        returned.reshape(experts * PACK, span), after, factor
    )


def solution(mesh):
    tokens = ("grp", "sp", "tp")
    return jax.shard_map(
        shards,
        mesh=mesh,
        in_specs=(
            P(tokens, None),
            P(("grp", "sp"), "tp"),
            P(("grp", "sp"), "tp"),
            P(None, "tp"),
            P("tp"),
            P("tp", None),
            P(),
            P(tokens, None),
            P(tokens, None),
            P(("sp", "tp"), None, None),
            P(("sp", "tp"), None, None),
            P(("sp", "tp"), None, None),
        ),
        out_specs=P(tokens, None),
        check_vma=False,
    )
```

```python
import jax
import jax.numpy as jnp
from jax import lax
from jax.experimental import pallas as pl
from jax.experimental.pallas import tpu as pltpu
from jax.sharding import PartitionSpec as P


F32 = jnp.float32
BF16 = jnp.bfloat16
HALO = 16
LANES = 128
PACK = 8
EXTRA = 16


def dot(a, b):
    return jnp.dot(a, b, preferred_element_type=F32)


def iota(shape, dim):
    return lax.broadcasted_iota(jnp.int32, shape, dim)


def gate(value, gating):
    return (value.astype(F32) * jax.nn.sigmoid(gating.astype(F32))).astype(BF16)


def terms(value):
    high = value.astype(BF16)
    rest = value - high.astype(F32)
    middle = rest.astype(BF16)
    return high, middle, (rest - middle.astype(F32)).astype(BF16)


def joined(block_ref, j, first):
    rows = [block_ref[j, first + k : first + k + 1, :].astype(F32) for k in range(3)]
    return rows[0] + rows[1] + rows[2]


def conv_kernel(rows_ref, low_ref, high_ref, table_ref, out_ref, pad_ref, sum_ref):
    taps, width = table_ref.shape[0] - 1, table_ref.shape[1]
    rows = rows_ref.shape[0]
    owners, owner_rows = out_ref.shape[0], out_ref.shape[1] - EXTRA
    step = 64
    parts = [slice(first, first + LANES) for first in range(0, width, LANES)]
    for part, lanes in enumerate(parts):
        pad_ref[part, 0:HALO] = low_ref[:, lanes].astype(F32)
        pad_ref[part, HALO : HALO + rows] = rows_ref[:, lanes].astype(F32)
        pad_ref[part, HALO + rows :] = high_ref[:, lanes].astype(F32)
    for part, lanes in enumerate(parts):
        for start in range(0, rows, step):
            total = jnp.zeros((step, LANES), F32)
            for tap in range(taps):
                first = start + HALO - taps // 2 + tap
                total = total + table_ref[tap : tap + 1, lanes] * pad_ref[part, first : first + step]
            sum_ref[start : start + step, lanes] = total
    gains = terms(table_ref[taps:, :])
    spare = jnp.zeros((EXTRA - 6, width), BF16)
    for owner in range(owners):
        block = sum_ref[owner * owner_rows : (owner + 1) * owner_rows]
        mean = jnp.sum(block, axis=1, keepdims=True) / width
        out_ref[owner, :owner_rows] = (block - mean).astype(BF16)
        across = jnp.transpose(jnp.broadcast_to(mean, (owner_rows, owner_rows)))[:1]
        across = jnp.concatenate([across, jnp.zeros((1, width - owner_rows), F32)], axis=1)
        out_ref[owner, owner_rows:] = jnp.concatenate([*gains, *terms(across), spare], axis=0)


def slots(ids_ref, experts):
    tokens = ids_ref.shape[1]
    expert = iota((experts, tokens), 0)
    chosen = jnp.zeros((experts, tokens), F32)
    for k in range(ids_ref.shape[0]):
        chosen = jnp.where(ids_ref[k : k + 1, :] == expert, 1.0, chosen)
    before = (iota((tokens, tokens), 0) < iota((tokens, tokens), 1)).astype(F32).astype(BF16)
    earlier = dot(chosen.astype(BF16), before)
    return jnp.where(chosen > 0, earlier + 1.0, 0.0)


def routing_kernel(ids_ref, weights_ref, pick_ref, factor_ref):
    rows = ids_ref.shape[1]
    size = pick_ref.shape[0]
    parts = pick_ref.shape[1] // rows
    cap = PACK // parts
    experts = size // PACK
    slot = slots(ids_ref, experts)
    expert = iota((experts, rows), 0)
    weight = jnp.zeros((experts, rows), F32)
    for k in range(ids_ref.shape[0]):
        weight = jnp.where(ids_ref[k : k + 1, :] == expert, weights_ref[k : k + 1, :], weight)
    weight = jnp.transpose(weight)
    coarse = weight.astype(BF16)
    fine = (weight - coarse.astype(F32)).astype(BF16)
    across = jnp.transpose(slot).astype(BF16)
    slot = slot.astype(BF16)
    block = 2 * LANES
    for start in range(0, size, block):
        row = iota((block, experts), 0) + start
        spread = ((row >> 3) == iota((block, experts), 1)).astype(F32).astype(BF16)
        wanted = dot(spread, slot)
        row = iota((block, rows), 0)
        hit = wanted == ((row & (cap - 1)) + 1).astype(F32)
        for part in range(parts):
            here = hit & (((row & (PACK - 1)) // cap) == part)
            pick_ref[start : start + block, part * rows : (part + 1) * rows] = here.astype(F32).astype(BF16)
    spread = (iota((experts, size), 0) == (iota((experts, size), 1) >> 3)).astype(F32).astype(BF16)
    column = iota((rows, size), 1)
    hit = dot(across, spread) == ((column & (cap - 1)) + 1).astype(F32)
    coarse, fine = dot(coarse, spread), dot(fine, spread)
    for part in range(parts):
        here = hit & (((column & (PACK - 1)) // cap) == part)
        for k, value in enumerate((coarse, fine)):
            first = (2 * part + k) * rows
            factor_ref[first : first + rows] = jnp.where(here, value, 0.0).astype(BF16)


def halves_kernel(place_ref, weights_hbm, first_ref, second_ref, sems):
    rows = first_ref.shape[0]
    core = place_ref[1]
    copies = []
    for k, (half, out_ref) in enumerate(((core, first_ref), (1 - core, second_ref))):
        source = weights_hbm.at[pl.ds(pl.multiple_of(half * rows, rows), rows)]
        copies.append(pltpu.make_async_copy(source, out_ref, sems.at[k]))
    for copy in copies:
        copy.start()
    for copy in copies:
        copy.wait()


def partial_kernel(
    place_ref, mixed_ref, own_ref, near_a_ref, near_b_ref, far_a_ref, far_b_ref, half_ref,
    out_ref, rest_ref, value_ref, act_ref,
):
    owners, _, width = mixed_ref.shape
    rows, features = out_ref.shape
    half_width = width // 2
    total = jnp.zeros((rows, 1), F32)
    for j in range(owners):
        across = joined(mixed_ref, j, rows + 3)[:, :rows]
        mean = jnp.transpose(jnp.broadcast_to(across, (rows, rows)))[:, :1]
        value_ref[j] = mixed_ref[j, :rows, :].astype(F32) + mean
        total = total + jnp.sum(value_ref[j], axis=1, keepdims=True)
    center = total / (owners * width)
    squares = jnp.zeros((rows, 1), F32)
    for j in range(owners):
        value = value_ref[j] - center
        squares = squares + jnp.sum(value * value, axis=1, keepdims=True)
    scale = lax.rsqrt(squares / (owners * width) + 0.05)
    for j in range(owners):
        value = (value_ref[j] - center) * scale * joined(mixed_ref, j, rows)
        value = (value * jax.nn.sigmoid(value)).astype(BF16)
        act_ref[2 * j] = value[:, :half_width]
        act_ref[2 * j + 1] = value[:, half_width:]
    place, core = place_ref[0], place_ref[1]
    before = 2 * lax.rem(place + owners - 1 + 2 * core, owners)
    beyond = 2 * lax.rem(place + owners + 1 - 2 * core, owners)
    across = 2 * lax.rem(place + 2, owners)
    rest_ref[...] = act_ref[across + 1 - core]
    pieces = (
        (before + core, near_a_ref), (before + 1 - core, near_b_ref),
        (beyond + 1 - core, far_a_ref), (beyond + core, far_b_ref), (across + core, half_ref),
    )
    step = 512
    for start in range(0, features, step):
        cols = slice(start, start + step)
        branch = dot(act_ref[2 * place], own_ref[:half_width, cols])
        branch = branch + dot(act_ref[2 * place + 1], own_ref[half_width:, cols])
        for index, piece_ref in pieces:
            branch = branch + dot(act_ref[index], piece_ref[:, cols])
        out_ref[:, cols] = branch


def dispatch_kernel(
    latents_ref, partial_ref, act_ref, rest_ref, gain_ref, pick_ref, after_ref, box_ref, x_ref
):
    rows, features = latents_ref.shape
    step = 512
    squares = jnp.zeros((rows, 1), F32)
    for start in range(0, features, step):
        cols = slice(start, start + step)
        branch = partial_ref[:, cols] + dot(act_ref[...], rest_ref[:, cols])
        after = (latents_ref[:, cols].astype(F32) + branch).astype(BF16)
        after_ref[:, cols] = after
        after = after.astype(F32)
        squares = squares + jnp.sum(after * after, axis=1, keepdims=True)
    scale = lax.rsqrt(squares / features + 0.01)
    parts = x_ref.shape[0] // rows
    span = features // parts
    for part in range(parts):
        cols = slice(part * span, (part + 1) * span)
        value = after_ref[:, cols].astype(F32) * scale * gain_ref[:, cols]
        x_ref[part * rows : (part + 1) * rows] = value.astype(BF16)
    block = 2 * LANES
    for start in range(0, box_ref.shape[0], block):
        box_ref[start : start + block] = dot(pick_ref[start : start + block], x_ref[...]).astype(BF16)


def shuffle_matrix(size, parts, inverse):
    cap = PACK // parts
    sources = size // PACK
    packed = iota((size, size), 0 if inverse else 1)
    split = iota((size, size), 1 if inverse else 0)
    source, part, slot = packed >> 3, (packed & (PACK - 1)) // cap, packed & (cap - 1)
    return ((part * sources + source) * cap + slot == split).astype(F32).astype(BF16)


def expert_kernel(in_ref, gate_ref, up_ref, down_ref, out_ref, x_ref, hidden_ref, y_ref):
    parts, rows, span = x_ref.shape
    block = 2 * LANES
    sub = block // parts
    forward = shuffle_matrix(block, parts, False)
    for i in range(in_ref.shape[0] // block):
        moved = dot(forward, in_ref[i * block : (i + 1) * block]).astype(BF16)
        for part in range(parts):
            x_ref[part, i * sub : (i + 1) * sub] = moved[part * sub : (part + 1) * sub]
    hidden_width = gate_ref.shape[1]
    tile = 256

    def inner(n, carry):
        cols = pl.ds(pl.multiple_of(n * tile, tile), tile)
        gated = jnp.zeros((rows, tile), F32)
        upped = jnp.zeros((rows, tile), F32)
        for part in range(parts):
            at = slice(part * span, (part + 1) * span)
            gated = gated + dot(x_ref[part], gate_ref[at, cols])
            upped = upped + dot(x_ref[part], up_ref[at, cols])
        hidden_ref[:, cols] = (gated * jax.nn.sigmoid(gated) * upped).astype(BF16)
        return carry

    lax.fori_loop(0, hidden_width // tile, inner, 0, unroll=True)
    for part in range(parts):

        def outer(n, carry, part=part):
            cols = pl.ds(pl.multiple_of(n * tile, tile), tile)
            weights = down_ref[:, pl.ds(pl.multiple_of(part * span + n * tile, tile), tile)]
            y_ref[part, :, cols] = dot(hidden_ref[...], weights).astype(BF16)
            return carry

        lax.fori_loop(0, span // tile, outer, 0, unroll=True)
    backward = shuffle_matrix(block, parts, True)
    for i in range(in_ref.shape[0] // block):
        stacked = jnp.concatenate(
            [y_ref[part, i * sub : (i + 1) * sub] for part in range(parts)], axis=0
        )
        out_ref[i * block : (i + 1) * block] = dot(backward, stacked).astype(BF16)


def combine_kernel(in_ref, after_ref, factor_ref, out_ref):
    rows, features = after_ref.shape
    span = in_ref.shape[1]
    for part in range(features // span):
        sums = dot(factor_ref[2 * part * rows : 2 * (part + 1) * rows], in_ref[...])
        cols = slice(part * span, (part + 1) * span)
        out_ref[:, cols] = (after_ref[:, cols].astype(F32) + (sums[:rows] + sums[rows:])).astype(BF16)


VMEM = pl.BlockSpec(memory_space=pltpu.VMEM)
SMEM = pl.BlockSpec(memory_space=pltpu.SMEM)
ANY = pl.BlockSpec(memory_space=pl.ANY)


def call(kernel, specs, outs, scratch, flops, size):
    return pl.pallas_call(
        kernel,
        in_specs=specs,
        out_specs=VMEM if not isinstance(outs, (list, tuple)) else [VMEM] * len(outs),
        out_shape=outs,
        scratch_shapes=scratch,
        compiler_params=pltpu.CompilerParams(vmem_limit_bytes=size << 20),
        cost_estimate=pl.CostEstimate(flops=flops, bytes_accessed=1 << 20, transcendentals=0),
    )


def shards(
    latents, conv_value, conv_gate, conv_taps, conv_gain, point_weight, channel_gain,
    expert_ids, expert_weights, gate_weight, up_weight, down_weight,
):
    shape = jax.ShapeDtypeStruct
    rows, features = latents.shape
    block_rows, width = conv_value.shape
    owners = lax.axis_size("tp")
    stages = lax.axis_size("sp")
    members = owners * stages
    top_count = expert_ids.shape[1]
    experts = gate_weight.shape[0] * members
    cap = 2 * top_count * rows // experts
    parts = PACK // cap
    span = features // parts

    ahead = [(i, i + 1) for i in range(stages - 1)]
    behind = [(i + 1, i) for i in range(stages - 1)]
    low = lax.ppermute(gate(conv_value[-HALO:], conv_gate[-HALO:]), "sp", ahead)
    high = lax.ppermute(gate(conv_value[:HALO], conv_gate[:HALO]), "sp", behind)

    place = lax.axis_index("tp")
    core = lax.rem(lax.axis_index("sp"), 2)
    half_width = width // 2
    aside = [
        (stage * owners + i, stage * owners + (i + (1, owners - 1)[stage % 2]) % owners)
        for stage in range(stages)
        for i in range(owners)
    ]
    swap = [(i, i ^ 1) for i in range(stages)]
    whereabouts = jnp.stack([place, core])
    piece = shape((half_width, features), BF16)
    leading, trailing = call(
        halves_kernel, [SMEM, ANY], [piece, piece], [pltpu.SemaphoreType.DMA((2,))], 10**6, 4
    )(whereabouts, point_weight)
    near_a = lax.ppermute(leading, ("sp", "tp"), aside)
    near_b = lax.ppermute(trailing, ("sp", "tp"), aside)

    gated = gate(conv_value, conv_gate)
    table = jnp.concatenate([conv_taps, conv_gain[None, :]], axis=0)
    sent = call(
        conv_kernel, [VMEM] * 4, shape((owners, rows + EXTRA, width), BF16),
        [
            pltpu.VMEM((width // LANES, block_rows + 2 * HALO, LANES), F32),
            pltpu.VMEM((block_rows, width), F32),
        ],
        10**9, 8,
    )(gated, low, high, table)
    near_a, _ = lax.optimization_barrier((near_a, sent))
    half = lax.ppermute(near_a, ("sp", "tp"), aside)
    far_a = lax.ppermute(near_a, "sp", swap)
    far_b = lax.ppermute(near_b, "sp", swap)
    rest = lax.ppermute(half, "sp", swap)
    mixed = lax.all_to_all(sent, "tp", split_axis=0, concat_axis=0, tiled=True)

    ids, weights, _ = lax.optimization_barrier((expert_ids.T, expert_weights.T, sent))
    pick, factor = call(
        routing_kernel, [VMEM] * 2,
        [shape((experts * PACK, parts * rows), BF16), shape((2 * parts * rows, experts * PACK), BF16)],
        [], 10**9, 8,
    )(ids, weights)
    partial, act = call(
        partial_kernel, [SMEM] + [VMEM] * 7,
        [shape((rows, features), F32), shape((rows, half_width), BF16)],
        [pltpu.VMEM((owners, rows, width), F32), pltpu.VMEM((2 * owners, rows, half_width), BF16)],
        10**9, 8,
    )(whereabouts, mixed, point_weight, near_a, near_b, far_a, far_b, half)
    after, box = call(
        dispatch_kernel, [VMEM] * 6,
        [shape((rows, features), BF16), shape((experts * PACK, span), BF16)],
        [pltpu.VMEM((parts * rows, span), BF16)], 10**9, 8,
    )(latents, partial, act, rest, channel_gain[None, :], pick)

    box = box.reshape(members, PACK, span)
    arrived = lax.all_to_all(box, ("sp", "tp"), split_axis=0, concat_axis=0, tiled=True)
    hidden_width = gate_weight.shape[2]
    answer = call(
        expert_kernel, [VMEM] * 4, shape((members * PACK, span), BF16),
        [
            pltpu.VMEM((parts, members * cap, span), BF16),
            pltpu.VMEM((members * cap, hidden_width), BF16),
            pltpu.VMEM((parts, members * cap, span), BF16),
        ],
        5 * 10**9, 12,
    )(arrived.reshape(members * PACK, span), gate_weight[0], up_weight[0], down_weight[0])
    answer = answer.reshape(members, PACK, span)
    returned = lax.all_to_all(answer, ("sp", "tp"), split_axis=0, concat_axis=0, tiled=True)
    return call(combine_kernel, [VMEM] * 3, shape((rows, features), BF16), [], 10**9, 8)(
        returned.reshape(experts * PACK, span), after, factor
    )


def solution(mesh):
    tokens = ("grp", "sp", "tp")
    return jax.shard_map(
        shards,
        mesh=mesh,
        in_specs=(
            P(tokens, None),
            P(("grp", "sp"), "tp"),
            P(("grp", "sp"), "tp"),
            P(None, "tp"),
            P("tp"),
            P("tp", None),
            P(),
            P(tokens, None),
            P(tokens, None),
            P(("sp", "tp"), None, None),
            P(("sp", "tp"), None, None),
            P(("sp", "tp"), None, None),
        ),
        out_specs=P(tokens, None),
        check_vma=False,
    )
```

```python
import jax
import jax.numpy as jnp
from jax import lax
from jax.experimental import pallas as pl
from jax.experimental.pallas import tpu as pltpu
from jax.sharding import PartitionSpec as P


F32 = jnp.float32
BF16 = jnp.bfloat16
HALO = 16
LANES = 128
PACK = 8
EXTRA = 16


def dot(a, b):
    return jnp.dot(a, b, preferred_element_type=F32)


def iota(shape, dim):
    return lax.broadcasted_iota(jnp.int32, shape, dim)


def gate(value, gating):
    return (value.astype(F32) * jax.nn.sigmoid(gating.astype(F32))).astype(BF16)


def terms(value):
    high = value.astype(BF16)
    rest = value - high.astype(F32)
    middle = rest.astype(BF16)
    return high, middle, (rest - middle.astype(F32)).astype(BF16)


def joined(block_ref, j, first):
    rows = [block_ref[j, first + k : first + k + 1, :].astype(F32) for k in range(3)]
    return rows[0] + rows[1] + rows[2]


def conv_kernel(rows_ref, low_ref, high_ref, table_ref, out_ref, pad_ref, sum_ref):
    taps, width = table_ref.shape[0] - 1, table_ref.shape[1]
    rows = rows_ref.shape[0]
    owners, owner_rows = out_ref.shape[0], out_ref.shape[1] - EXTRA
    step = 64
    parts = [slice(first, first + LANES) for first in range(0, width, LANES)]
    for part, lanes in enumerate(parts):
        pad_ref[part, 0:HALO] = low_ref[:, lanes].astype(F32)
        pad_ref[part, HALO : HALO + rows] = rows_ref[:, lanes].astype(F32)
        pad_ref[part, HALO + rows :] = high_ref[:, lanes].astype(F32)
    for part, lanes in enumerate(parts):
        for start in range(0, rows, step):
            total = jnp.zeros((step, LANES), F32)
            for tap in range(taps):
                first = start + HALO - taps // 2 + tap
                total = total + table_ref[tap : tap + 1, lanes] * pad_ref[part, first : first + step]
            sum_ref[start : start + step, lanes] = total
    gains = terms(table_ref[taps:, :])
    spare = jnp.zeros((EXTRA - 6, width), BF16)
    for owner in range(owners):
        block = sum_ref[owner * owner_rows : (owner + 1) * owner_rows]
        mean = jnp.sum(block, axis=1, keepdims=True) / width
        out_ref[owner, :owner_rows] = (block - mean).astype(BF16)
        across = jnp.transpose(jnp.broadcast_to(mean, (owner_rows, owner_rows)))[:1]
        across = jnp.concatenate([across, jnp.zeros((1, width - owner_rows), F32)], axis=1)
        out_ref[owner, owner_rows:] = jnp.concatenate([*gains, *terms(across), spare], axis=0)


def slots(ids_ref, experts):
    tokens = ids_ref.shape[1]
    expert = iota((experts, tokens), 0)
    chosen = jnp.zeros((experts, tokens), F32)
    for k in range(ids_ref.shape[0]):
        chosen = jnp.where(ids_ref[k : k + 1, :] == expert, 1.0, chosen)
    before = (iota((tokens, tokens), 0) < iota((tokens, tokens), 1)).astype(F32).astype(BF16)
    earlier = dot(chosen.astype(BF16), before)
    return jnp.where(chosen > 0, earlier + 1.0, 0.0)


def routing_kernel(ids_ref, weights_ref, pick_ref, factor_ref):
    rows = ids_ref.shape[1]
    size = pick_ref.shape[0]
    parts = pick_ref.shape[1] // rows
    cap = PACK // parts
    experts = size // PACK
    slot = slots(ids_ref, experts)
    expert = iota((experts, rows), 0)
    weight = jnp.zeros((experts, rows), F32)
    for k in range(ids_ref.shape[0]):
        weight = jnp.where(ids_ref[k : k + 1, :] == expert, weights_ref[k : k + 1, :], weight)
    weight = jnp.transpose(weight)
    coarse = weight.astype(BF16)
    fine = (weight - coarse.astype(F32)).astype(BF16)
    across = jnp.transpose(slot).astype(BF16)
    slot = slot.astype(BF16)
    block = 2 * LANES
    for start in range(0, size, block):
        row = iota((block, experts), 0) + start
        spread = ((row >> 3) == iota((block, experts), 1)).astype(F32).astype(BF16)
        wanted = dot(spread, slot)
        row = iota((block, rows), 0)
        hit = wanted == ((row & (cap - 1)) + 1).astype(F32)
        for part in range(parts):
            here = hit & (((row & (PACK - 1)) // cap) == part)
            pick_ref[start : start + block, part * rows : (part + 1) * rows] = here.astype(F32).astype(BF16)
    spread = (iota((experts, size), 0) == (iota((experts, size), 1) >> 3)).astype(F32).astype(BF16)
    column = iota((rows, size), 1)
    hit = dot(across, spread) == ((column & (cap - 1)) + 1).astype(F32)
    coarse, fine = dot(coarse, spread), dot(fine, spread)
    for part in range(parts):
        here = hit & (((column & (PACK - 1)) // cap) == part)
        for k, value in enumerate((coarse, fine)):
            first = (2 * part + k) * rows
            factor_ref[first : first + rows] = jnp.where(here, value, 0.0).astype(BF16)


def partial_kernel(
    place_ref, mixed_ref, own_ref, near_ref, swapped_ref, out_ref, first_ref, second_ref, value_ref, act_ref
):
    owners, _, width = mixed_ref.shape
    rows, features = out_ref.shape
    half_width = width // 2
    total = jnp.zeros((rows, 1), F32)
    for j in range(owners):
        across = joined(mixed_ref, j, rows + 3)[:, :rows]
        mean = jnp.transpose(jnp.broadcast_to(across, (rows, rows)))[:, :1]
        value_ref[j] = mixed_ref[j, :rows, :].astype(F32) + mean
        total = total + jnp.sum(value_ref[j], axis=1, keepdims=True)
    center = total / (owners * width)
    squares = jnp.zeros((rows, 1), F32)
    for j in range(owners):
        value = value_ref[j] - center
        squares = squares + jnp.sum(value * value, axis=1, keepdims=True)
    scale = lax.rsqrt(squares / (owners * width) + 0.05)
    for j in range(owners):
        value = (value_ref[j] - center) * scale * joined(mixed_ref, j, rows)
        act_ref[j] = (value * jax.nn.sigmoid(value)).astype(BF16)
    place, core = place_ref[0], place_ref[1]
    before = lax.rem(place + owners - 1 + 2 * core, owners)
    beyond = lax.rem(place + owners + 1 - 2 * core, owners)
    across = act_ref[lax.rem(place + 2, owners)]
    lower, upper = across[:, :half_width], across[:, half_width:]
    first_ref[...] = jnp.where(core == 0, lower, upper)
    second_ref[...] = jnp.where(core == 0, upper, lower)
    step = 512
    for start in range(0, features, step):
        cols = slice(start, start + step)
        branch = dot(act_ref[place], own_ref[:, cols])
        branch = branch + dot(act_ref[before], near_ref[:, cols])
        out_ref[:, cols] = branch + dot(act_ref[beyond], swapped_ref[:, cols])


def dispatch_kernel(
    latents_ref, partial_ref, first_ref, second_ref, half_ref, rest_ref, gain_ref, pick_ref,
    after_ref, box_ref, x_ref,
):
    rows, features = latents_ref.shape
    step = 512
    squares = jnp.zeros((rows, 1), F32)
    for start in range(0, features, step):
        cols = slice(start, start + step)
        branch = partial_ref[:, cols] + dot(first_ref[...], half_ref[:, cols])
        branch = branch + dot(second_ref[...], rest_ref[:, cols])
        after = (latents_ref[:, cols].astype(F32) + branch).astype(BF16)
        after_ref[:, cols] = after
        after = after.astype(F32)
        squares = squares + jnp.sum(after * after, axis=1, keepdims=True)
    scale = lax.rsqrt(squares / features + 0.01)
    parts = x_ref.shape[0] // rows
    span = features // parts
    for part in range(parts):
        cols = slice(part * span, (part + 1) * span)
        value = after_ref[:, cols].astype(F32) * scale * gain_ref[:, cols]
        x_ref[part * rows : (part + 1) * rows] = value.astype(BF16)
    block = 2 * LANES
    for start in range(0, box_ref.shape[0], block):
        box_ref[start : start + block] = dot(pick_ref[start : start + block], x_ref[...]).astype(BF16)


def shuffle_matrix(size, parts, inverse):
    cap = PACK // parts
    sources = size // PACK
    packed = iota((size, size), 0 if inverse else 1)
    split = iota((size, size), 1 if inverse else 0)
    source, part, slot = packed >> 3, (packed & (PACK - 1)) // cap, packed & (cap - 1)
    return ((part * sources + source) * cap + slot == split).astype(F32).astype(BF16)


def expert_kernel(in_ref, gate_ref, up_ref, down_ref, out_ref, x_ref, hidden_ref, y_ref):
    parts, rows, span = x_ref.shape
    block = 2 * LANES
    sub = block // parts
    forward = shuffle_matrix(block, parts, False)
    for i in range(in_ref.shape[0] // block):
        moved = dot(forward, in_ref[i * block : (i + 1) * block]).astype(BF16)
        for part in range(parts):
            x_ref[part, i * sub : (i + 1) * sub] = moved[part * sub : (part + 1) * sub]
    hidden_width = gate_ref.shape[1]
    tile = 256

    def inner(n, carry):
        cols = pl.ds(pl.multiple_of(n * tile, tile), tile)
        gated = jnp.zeros((rows, tile), F32)
        upped = jnp.zeros((rows, tile), F32)
        for part in range(parts):
            at = slice(part * span, (part + 1) * span)
            gated = gated + dot(x_ref[part], gate_ref[at, cols])
            upped = upped + dot(x_ref[part], up_ref[at, cols])
        hidden_ref[:, cols] = (gated * jax.nn.sigmoid(gated) * upped).astype(BF16)
        return carry

    lax.fori_loop(0, hidden_width // tile, inner, 0, unroll=True)
    for part in range(parts):

        def outer(n, carry, part=part):
            cols = pl.ds(pl.multiple_of(n * tile, tile), tile)
            weights = down_ref[:, pl.ds(pl.multiple_of(part * span + n * tile, tile), tile)]
            y_ref[part, :, cols] = dot(hidden_ref[...], weights).astype(BF16)
            return carry

        lax.fori_loop(0, span // tile, outer, 0, unroll=True)
    backward = shuffle_matrix(block, parts, True)
    for i in range(in_ref.shape[0] // block):
        stacked = jnp.concatenate(
            [y_ref[part, i * sub : (i + 1) * sub] for part in range(parts)], axis=0
        )
        out_ref[i * block : (i + 1) * block] = dot(backward, stacked).astype(BF16)


def combine_kernel(in_ref, after_ref, factor_ref, out_ref):
    rows, features = after_ref.shape
    span = in_ref.shape[1]
    for part in range(features // span):
        sums = dot(factor_ref[2 * part * rows : 2 * (part + 1) * rows], in_ref[...])
        cols = slice(part * span, (part + 1) * span)
        out_ref[:, cols] = (after_ref[:, cols].astype(F32) + (sums[:rows] + sums[rows:])).astype(BF16)


VMEM = pl.BlockSpec(memory_space=pltpu.VMEM)
SMEM = pl.BlockSpec(memory_space=pltpu.SMEM)


def call(kernel, specs, outs, scratch, flops, size):
    return pl.pallas_call(
        kernel,
        in_specs=specs,
        out_specs=VMEM if not isinstance(outs, (list, tuple)) else [VMEM] * len(outs),
        out_shape=outs,
        scratch_shapes=scratch,
        compiler_params=pltpu.CompilerParams(vmem_limit_bytes=size << 20),
        cost_estimate=pl.CostEstimate(flops=flops, bytes_accessed=1 << 20, transcendentals=0),
    )


def shards(
    latents, conv_value, conv_gate, conv_taps, conv_gain, point_weight, channel_gain,
    expert_ids, expert_weights, gate_weight, up_weight, down_weight,
):
    shape = jax.ShapeDtypeStruct
    rows, features = latents.shape
    block_rows, width = conv_value.shape
    owners = lax.axis_size("tp")
    stages = lax.axis_size("sp")
    members = owners * stages
    top_count = expert_ids.shape[1]
    experts = gate_weight.shape[0] * members
    cap = 2 * top_count * rows // experts
    parts = PACK // cap
    span = features // parts

    ahead = [(i, i + 1) for i in range(stages - 1)]
    behind = [(i + 1, i) for i in range(stages - 1)]
    low = lax.ppermute(gate(conv_value[-HALO:], conv_gate[-HALO:]), "sp", ahead)
    high = lax.ppermute(gate(conv_value[:HALO], conv_gate[:HALO]), "sp", behind)

    place = lax.axis_index("tp")
    core = lax.rem(lax.axis_index("sp"), 2)
    half_width = width // 2
    aside = [
        (stage * owners + i, stage * owners + (i + (1, owners - 1)[stage % 2]) % owners)
        for stage in range(stages)
        for i in range(owners)
    ]
    swap = [(i, i ^ 1) for i in range(stages)]
    near = lax.ppermute(point_weight, ("sp", "tp"), aside)

    gated = gate(conv_value, conv_gate)
    table = jnp.concatenate([conv_taps, conv_gain[None, :]], axis=0)
    sent = call(
        conv_kernel, [VMEM] * 4, shape((owners, rows + EXTRA, width), BF16),
        [
            pltpu.VMEM((width // LANES, block_rows + 2 * HALO, LANES), F32),
            pltpu.VMEM((block_rows, width), F32),
        ],
        10**9, 8,
    )(gated, low, high, table)
    near, _ = lax.optimization_barrier((near, sent))
    half = lax.dynamic_slice_in_dim(near, core * half_width, half_width, 0)
    half = lax.ppermute(half, ("sp", "tp"), aside)
    swapped = lax.ppermute(near, "sp", swap)
    rest = lax.ppermute(half, "sp", swap)
    mixed = lax.all_to_all(sent, "tp", split_axis=0, concat_axis=0, tiled=True)

    ids, weights, _ = lax.optimization_barrier((expert_ids.T, expert_weights.T, sent))
    pick, factor = call(
        routing_kernel, [VMEM] * 2,
        [shape((experts * PACK, parts * rows), BF16), shape((2 * parts * rows, experts * PACK), BF16)],
        [], 10**9, 8,
    )(ids, weights)
    partial, first, second = call(
        partial_kernel, [SMEM] + [VMEM] * 4,
        [shape((rows, features), F32)] + [shape((rows, half_width), BF16)] * 2,
        [pltpu.VMEM((owners, rows, width), F32), pltpu.VMEM((owners, rows, width), BF16)],
        10**9, 8,
    )(jnp.stack([place, core]), mixed, point_weight, near, swapped)
    after, box = call(
        dispatch_kernel, [VMEM] * 8,
        [shape((rows, features), BF16), shape((experts * PACK, span), BF16)],
        [pltpu.VMEM((parts * rows, span), BF16)], 10**9, 8,
    )(latents, partial, first, second, half, rest, channel_gain[None, :], pick)

    box = box.reshape(members, PACK, span)
    arrived = lax.all_to_all(box, ("sp", "tp"), split_axis=0, concat_axis=0, tiled=True)
    hidden_width = gate_weight.shape[2]
    answer = call(
        expert_kernel, [VMEM] * 4, shape((members * PACK, span), BF16),
        [
            pltpu.VMEM((parts, members * cap, span), BF16),
            pltpu.VMEM((members * cap, hidden_width), BF16),
            pltpu.VMEM((parts, members * cap, span), BF16),
        ],
        5 * 10**9, 12,
    )(arrived.reshape(members * PACK, span), gate_weight[0], up_weight[0], down_weight[0])
    answer = answer.reshape(members, PACK, span)
    returned = lax.all_to_all(answer, ("sp", "tp"), split_axis=0, concat_axis=0, tiled=True)
    return call(combine_kernel, [VMEM] * 3, shape((rows, features), BF16), [], 10**9, 8)(
        returned.reshape(experts * PACK, span), after, factor
    )


def solution(mesh):
    tokens = ("grp", "sp", "tp")
    return jax.shard_map(
        shards,
        mesh=mesh,
        in_specs=(
            P(tokens, None),
            P(("grp", "sp"), "tp"),
            P(("grp", "sp"), "tp"),
            P(None, "tp"),
            P("tp"),
            P("tp", None),
            P(),
            P(tokens, None),
            P(tokens, None),
            P(("sp", "tp"), None, None),
            P(("sp", "tp"), None, None),
            P(("sp", "tp"), None, None),
        ),
        out_specs=P(tokens, None),
        check_vma=False,
    )
```

```python
import jax
import jax.numpy as jnp
from jax import lax
from jax.experimental import pallas as pl
from jax.experimental.pallas import tpu as pltpu
from jax.sharding import PartitionSpec as P


F32 = jnp.float32
BF16 = jnp.bfloat16
HALO = 16
LANES = 128
PACK = 8
EXTRA = 16


def dot(a, b):
    return jnp.dot(a, b, preferred_element_type=F32)


def iota(shape, dim):
    return lax.broadcasted_iota(jnp.int32, shape, dim)


def gate(value, gating):
    return (value.astype(F32) * jax.nn.sigmoid(gating.astype(F32))).astype(BF16)


def terms(value):
    high = value.astype(BF16)
    rest = value - high.astype(F32)
    middle = rest.astype(BF16)
    return high, middle, (rest - middle.astype(F32)).astype(BF16)


def joined(block_ref, j, first):
    rows = [block_ref[j, first + k : first + k + 1, :].astype(F32) for k in range(3)]
    return rows[0] + rows[1] + rows[2]


def conv_kernel(rows_ref, low_ref, high_ref, table_ref, out_ref, pad_ref, sum_ref):
    taps, width = table_ref.shape[0] - 1, table_ref.shape[1]
    rows = rows_ref.shape[0]
    owners, owner_rows = out_ref.shape[0], out_ref.shape[1] - EXTRA
    step = 64
    parts = [slice(first, first + LANES) for first in range(0, width, LANES)]
    for part, lanes in enumerate(parts):
        pad_ref[part, 0:HALO] = low_ref[:, lanes].astype(F32)
        pad_ref[part, HALO : HALO + rows] = rows_ref[:, lanes].astype(F32)
        pad_ref[part, HALO + rows :] = high_ref[:, lanes].astype(F32)
    for part, lanes in enumerate(parts):
        for start in range(0, rows, step):
            total = jnp.zeros((step, LANES), F32)
            for tap in range(taps):
                first = start + HALO - taps // 2 + tap
                total = total + table_ref[tap : tap + 1, lanes] * pad_ref[part, first : first + step]
            sum_ref[start : start + step, lanes] = total
    gains = terms(table_ref[taps:, :])
    spare = jnp.zeros((EXTRA - 6, width), BF16)
    for owner in range(owners):
        block = sum_ref[owner * owner_rows : (owner + 1) * owner_rows]
        mean = jnp.sum(block, axis=1, keepdims=True) / width
        out_ref[owner, :owner_rows] = (block - mean).astype(BF16)
        across = jnp.transpose(jnp.broadcast_to(mean, (owner_rows, owner_rows)))[:1]
        across = jnp.concatenate([across, jnp.zeros((1, width - owner_rows), F32)], axis=1)
        out_ref[owner, owner_rows:] = jnp.concatenate([*gains, *terms(across), spare], axis=0)


def slots(ids_ref, experts):
    tokens = ids_ref.shape[1]
    expert = iota((experts, tokens), 0)
    chosen = jnp.zeros((experts, tokens), F32)
    for k in range(ids_ref.shape[0]):
        chosen = jnp.where(ids_ref[k : k + 1, :] == expert, 1.0, chosen)
    before = (iota((tokens, tokens), 0) < iota((tokens, tokens), 1)).astype(F32).astype(BF16)
    earlier = dot(chosen.astype(BF16), before)
    return jnp.where(chosen > 0, earlier + 1.0, 0.0)


def routing_kernel(ids_ref, weights_ref, pick_ref, factor_ref):
    rows = ids_ref.shape[1]
    size = pick_ref.shape[0]
    parts = pick_ref.shape[1] // rows
    cap = PACK // parts
    experts = size // PACK
    slot = slots(ids_ref, experts)
    expert = iota((experts, rows), 0)
    weight = jnp.zeros((experts, rows), F32)
    for k in range(ids_ref.shape[0]):
        weight = jnp.where(ids_ref[k : k + 1, :] == expert, weights_ref[k : k + 1, :], weight)
    weight = jnp.transpose(weight)
    coarse = weight.astype(BF16)
    fine = (weight - coarse.astype(F32)).astype(BF16)
    across = jnp.transpose(slot).astype(BF16)
    slot = slot.astype(BF16)
    block = 2 * LANES
    for start in range(0, size, block):
        row = iota((block, experts), 0) + start
        spread = ((row >> 3) == iota((block, experts), 1)).astype(F32).astype(BF16)
        wanted = dot(spread, slot)
        row = iota((block, rows), 0)
        hit = wanted == ((row & (cap - 1)) + 1).astype(F32)
        for part in range(parts):
            here = hit & (((row & (PACK - 1)) // cap) == part)
            pick_ref[start : start + block, part * rows : (part + 1) * rows] = here.astype(F32).astype(BF16)
    spread = (iota((experts, size), 0) == (iota((experts, size), 1) >> 3)).astype(F32).astype(BF16)
    column = iota((rows, size), 1)
    hit = dot(across, spread) == ((column & (cap - 1)) + 1).astype(F32)
    coarse, fine = dot(coarse, spread), dot(fine, spread)
    for part in range(parts):
        here = hit & (((column & (PACK - 1)) // cap) == part)
        for k, value in enumerate((coarse, fine)):
            first = (2 * part + k) * rows
            factor_ref[first : first + rows] = jnp.where(here, value, 0.0).astype(BF16)


def half_kernel(place_ref, block_ref, out_ref):
    rows = out_ref.shape[0]
    out_ref[...] = block_ref[pl.ds(pl.multiple_of(place_ref[1] * rows, rows), rows)]


def partial_kernel(
    place_ref, mixed_ref, own_ref, near_ref, swapped_ref, out_ref, first_ref, second_ref, value_ref, act_ref
):
    owners, _, width = mixed_ref.shape
    rows, features = out_ref.shape
    half_width = width // 2
    total = jnp.zeros((rows, 1), F32)
    for j in range(owners):
        across = joined(mixed_ref, j, rows + 3)[:, :rows]
        mean = jnp.transpose(jnp.broadcast_to(across, (rows, rows)))[:, :1]
        value_ref[j] = mixed_ref[j, :rows, :].astype(F32) + mean
        total = total + jnp.sum(value_ref[j], axis=1, keepdims=True)
    center = total / (owners * width)
    squares = jnp.zeros((rows, 1), F32)
    for j in range(owners):
        value = value_ref[j] - center
        squares = squares + jnp.sum(value * value, axis=1, keepdims=True)
    scale = lax.rsqrt(squares / (owners * width) + 0.05)
    for j in range(owners):
        value = (value_ref[j] - center) * scale * joined(mixed_ref, j, rows)
        act_ref[j] = (value * jax.nn.sigmoid(value)).astype(BF16)
    place, core = place_ref[0], place_ref[1]
    before = lax.rem(place + owners - 1 + 2 * core, owners)
    beyond = lax.rem(place + owners + 1 - 2 * core, owners)
    across = act_ref[lax.rem(place + 2, owners)]
    lower, upper = across[:, :half_width], across[:, half_width:]
    first_ref[...] = jnp.where(core == 0, lower, upper)
    second_ref[...] = jnp.where(core == 0, upper, lower)
    step = 512
    for start in range(0, features, step):
        cols = slice(start, start + step)
        branch = dot(act_ref[place], own_ref[:, cols])
        branch = branch + dot(act_ref[before], near_ref[:, cols])
        out_ref[:, cols] = branch + dot(act_ref[beyond], swapped_ref[:, cols])


def dispatch_kernel(
    latents_ref, partial_ref, first_ref, second_ref, half_ref, rest_ref, gain_ref, pick_ref,
    after_ref, box_ref, x_ref,
):
    rows, features = latents_ref.shape
    step = 512
    squares = jnp.zeros((rows, 1), F32)
    for start in range(0, features, step):
        cols = slice(start, start + step)
        branch = partial_ref[:, cols] + dot(first_ref[...], half_ref[:, cols])
        branch = branch + dot(second_ref[...], rest_ref[:, cols])
        after = (latents_ref[:, cols].astype(F32) + branch).astype(BF16)
        after_ref[:, cols] = after
        after = after.astype(F32)
        squares = squares + jnp.sum(after * after, axis=1, keepdims=True)
    scale = lax.rsqrt(squares / features + 0.01)
    parts = x_ref.shape[0] // rows
    span = features // parts
    for part in range(parts):
        cols = slice(part * span, (part + 1) * span)
        value = after_ref[:, cols].astype(F32) * scale * gain_ref[:, cols]
        x_ref[part * rows : (part + 1) * rows] = value.astype(BF16)
    block = 2 * LANES
    for start in range(0, box_ref.shape[0], block):
        box_ref[start : start + block] = dot(pick_ref[start : start + block], x_ref[...]).astype(BF16)


def shuffle_matrix(size, parts, inverse):
    cap = PACK // parts
    sources = size // PACK
    packed = iota((size, size), 0 if inverse else 1)
    split = iota((size, size), 1 if inverse else 0)
    source, part, slot = packed >> 3, (packed & (PACK - 1)) // cap, packed & (cap - 1)
    return ((part * sources + source) * cap + slot == split).astype(F32).astype(BF16)


def expert_kernel(in_ref, gate_ref, up_ref, down_ref, out_ref, x_ref, hidden_ref, y_ref):
    parts, rows, span = x_ref.shape
    block = 2 * LANES
    sub = block // parts
    forward = shuffle_matrix(block, parts, False)
    for i in range(in_ref.shape[0] // block):
        moved = dot(forward, in_ref[i * block : (i + 1) * block]).astype(BF16)
        for part in range(parts):
            x_ref[part, i * sub : (i + 1) * sub] = moved[part * sub : (part + 1) * sub]
    hidden_width = gate_ref.shape[1]
    tile = 256

    def inner(n, carry):
        cols = pl.ds(pl.multiple_of(n * tile, tile), tile)
        gated = jnp.zeros((rows, tile), F32)
        upped = jnp.zeros((rows, tile), F32)
        for part in range(parts):
            at = slice(part * span, (part + 1) * span)
            gated = gated + dot(x_ref[part], gate_ref[at, cols])
            upped = upped + dot(x_ref[part], up_ref[at, cols])
        hidden_ref[:, cols] = (gated * jax.nn.sigmoid(gated) * upped).astype(BF16)
        return carry

    lax.fori_loop(0, hidden_width // tile, inner, 0, unroll=True)
    for part in range(parts):

        def outer(n, carry, part=part):
            cols = pl.ds(pl.multiple_of(n * tile, tile), tile)
            weights = down_ref[:, pl.ds(pl.multiple_of(part * span + n * tile, tile), tile)]
            y_ref[part, :, cols] = dot(hidden_ref[...], weights).astype(BF16)
            return carry

        lax.fori_loop(0, span // tile, outer, 0, unroll=True)
    backward = shuffle_matrix(block, parts, True)
    for i in range(in_ref.shape[0] // block):
        stacked = jnp.concatenate(
            [y_ref[part, i * sub : (i + 1) * sub] for part in range(parts)], axis=0
        )
        out_ref[i * block : (i + 1) * block] = dot(backward, stacked).astype(BF16)


def combine_kernel(in_ref, after_ref, factor_ref, out_ref):
    rows, features = after_ref.shape
    span = in_ref.shape[1]
    for part in range(features // span):
        sums = dot(factor_ref[2 * part * rows : 2 * (part + 1) * rows], in_ref[...])
        cols = slice(part * span, (part + 1) * span)
        out_ref[:, cols] = (after_ref[:, cols].astype(F32) + (sums[:rows] + sums[rows:])).astype(BF16)


VMEM = pl.BlockSpec(memory_space=pltpu.VMEM)
SMEM = pl.BlockSpec(memory_space=pltpu.SMEM)


def call(kernel, specs, outs, scratch, flops, size):
    return pl.pallas_call(
        kernel,
        in_specs=specs,
        out_specs=VMEM if not isinstance(outs, (list, tuple)) else [VMEM] * len(outs),
        out_shape=outs,
        scratch_shapes=scratch,
        compiler_params=pltpu.CompilerParams(vmem_limit_bytes=size << 20),
        cost_estimate=pl.CostEstimate(flops=flops, bytes_accessed=1 << 20, transcendentals=0),
    )


def shards(
    latents, conv_value, conv_gate, conv_taps, conv_gain, point_weight, channel_gain,
    expert_ids, expert_weights, gate_weight, up_weight, down_weight,
):
    shape = jax.ShapeDtypeStruct
    rows, features = latents.shape
    block_rows, width = conv_value.shape
    owners = lax.axis_size("tp")
    stages = lax.axis_size("sp")
    members = owners * stages
    top_count = expert_ids.shape[1]
    experts = gate_weight.shape[0] * members
    cap = 2 * top_count * rows // experts
    parts = PACK // cap
    span = features // parts

    ahead = [(i, i + 1) for i in range(stages - 1)]
    behind = [(i + 1, i) for i in range(stages - 1)]
    low = lax.ppermute(gate(conv_value[-HALO:], conv_gate[-HALO:]), "sp", ahead)
    high = lax.ppermute(gate(conv_value[:HALO], conv_gate[:HALO]), "sp", behind)

    place = lax.axis_index("tp")
    core = lax.rem(lax.axis_index("sp"), 2)
    half_width = width // 2
    aside = [
        (stage * owners + i, stage * owners + (i + (1, owners - 1)[stage % 2]) % owners)
        for stage in range(stages)
        for i in range(owners)
    ]
    swap = [(i, i ^ 1) for i in range(stages)]
    near = lax.ppermute(point_weight, ("sp", "tp"), aside)

    gated = gate(conv_value, conv_gate)
    table = jnp.concatenate([conv_taps, conv_gain[None, :]], axis=0)
    sent = call(
        conv_kernel, [VMEM] * 4, shape((owners, rows + EXTRA, width), BF16),
        [
            pltpu.VMEM((width // LANES, block_rows + 2 * HALO, LANES), F32),
            pltpu.VMEM((block_rows, width), F32),
        ],
        10**9, 8,
    )(gated, low, high, table)
    near, _ = lax.optimization_barrier((near, sent))
    whereabouts = jnp.stack([place, core])
    half = call(half_kernel, [SMEM, VMEM], shape((half_width, features), BF16), [], 10**6, 4)(
        whereabouts, near
    )
    half = lax.ppermute(half, ("sp", "tp"), aside)
    swapped = lax.ppermute(near, "sp", swap)
    rest = lax.ppermute(half, "sp", swap)
    mixed = lax.all_to_all(sent, "tp", split_axis=0, concat_axis=0, tiled=True)

    ids, weights, _ = lax.optimization_barrier((expert_ids.T, expert_weights.T, sent))
    pick, factor = call(
        routing_kernel, [VMEM] * 2,
        [shape((experts * PACK, parts * rows), BF16), shape((2 * parts * rows, experts * PACK), BF16)],
        [], 10**9, 8,
    )(ids, weights)
    partial, first, second = call(
        partial_kernel, [SMEM] + [VMEM] * 4,
        [shape((rows, features), F32)] + [shape((rows, half_width), BF16)] * 2,
        [pltpu.VMEM((owners, rows, width), F32), pltpu.VMEM((owners, rows, width), BF16)],
        10**9, 8,
    )(whereabouts, mixed, point_weight, near, swapped)
    after, box = call(
        dispatch_kernel, [VMEM] * 8,
        [shape((rows, features), BF16), shape((experts * PACK, span), BF16)],
        [pltpu.VMEM((parts * rows, span), BF16)], 10**9, 8,
    )(latents, partial, first, second, half, rest, channel_gain[None, :], pick)

    box = box.reshape(members, PACK, span)
    arrived = lax.all_to_all(box, ("sp", "tp"), split_axis=0, concat_axis=0, tiled=True)
    hidden_width = gate_weight.shape[2]
    answer = call(
        expert_kernel, [VMEM] * 4, shape((members * PACK, span), BF16),
        [
            pltpu.VMEM((parts, members * cap, span), BF16),
            pltpu.VMEM((members * cap, hidden_width), BF16),
            pltpu.VMEM((parts, members * cap, span), BF16),
        ],
        5 * 10**9, 12,
    )(arrived.reshape(members * PACK, span), gate_weight[0], up_weight[0], down_weight[0])
    answer = answer.reshape(members, PACK, span)
    returned = lax.all_to_all(answer, ("sp", "tp"), split_axis=0, concat_axis=0, tiled=True)
    return call(combine_kernel, [VMEM] * 3, shape((rows, features), BF16), [], 10**9, 8)(
        returned.reshape(experts * PACK, span), after, factor
    )


def solution(mesh):
    tokens = ("grp", "sp", "tp")
    return jax.shard_map(
        shards,
        mesh=mesh,
        in_specs=(
            P(tokens, None),
            P(("grp", "sp"), "tp"),
            P(("grp", "sp"), "tp"),
            P(None, "tp"),
            P("tp"),
            P("tp", None),
            P(),
            P(tokens, None),
            P(tokens, None),
            P(("sp", "tp"), None, None),
            P(("sp", "tp"), None, None),
            P(("sp", "tp"), None, None),
        ),
        out_specs=P(tokens, None),
        check_vma=False,
    )
```
